128 devices in a mesh: sp: 32 (over z, y, core), tp: 4 (over x).
Axes of the slice: x: 4, y: 4, z: 4, core: 2. Of those that a mesh axis runs over, the one named last changes fastest.
Arguments:
- tokens: bfloat16 [32768, 2048], P(('sp', 'tp')), may hold values from -6 to 6
- norm_gain: float32 [2048], replicated, may hold values from 0.1 to 1.9
- w_query: bfloat16 [2048, 2048], P(None, 'tp'), may hold values from -0.125 to 0.125
- w_forget: bfloat16 [2048, 2048], P(None, 'tp'), may hold values from -0.125 to 0.125
- w_value: bfloat16 [2048, 2048], P(None, 'tp'), may hold values from -0.125 to 0.125
- w_rgate: bfloat16 [2048, 2048], P(None, 'tp'), may hold values from -0.125 to 0.125
- w_glu_value: bfloat16 [2048, 2048], P(None, 'tp'), may hold values from -0.125 to 0.125
- w_glu_gate: bfloat16 [2048, 2048], P(None, 'tp'), may hold values from -0.125 to 0.125
- forget_gap: float32 [2048], P('tp'), may hold values from 1.5258789e-05 to 0.1
- decay_shift: float32 [32768, 16], P('sp', 'tp'), may hold values from -0.6 to 0, as said below
- head_gain: float32 [128], replicated, may hold values from 0.1 to 1.9
- conv_taps: float32 [31, 2048], P(None, 'tp'), may hold values from -12 to 12
- conv_gain: float32 [2048], P('tp'), may hold values from 0.1 to 1.9
- out_rec: bfloat16 [2048, 2048], P('tp'), may hold values from -0.09375 to 0.09375
- out_conv: bfloat16 [2048, 2048], P('tp'), may hold values from -0.09375 to 0.09375
Outputs:
- mixed: bfloat16 [32768, 2048], P(('sp', 'tp'))
The draws below stay inside these ranges and needn't reach their ends.
Inputs may be any that keep to these rules, and one draw needn't show every extreme that they name: `decay_shift`: at most zero everywhere.
All inputs are finite; a program needn't handle non-finite values.
Results may differ from the reference program's by a relative error of at most 0.015.
Values may be sent and summed in bfloat16 or wider, within the bound.
No kernel may reach another device: no remote copies, remote signals or barrier semaphores. Data moves between devices by JAX's collectives and lax.ppermute only.
A program may use at most 128 MiB of HBM per device.

```python
import jax
import jax.numpy as jnp
from jax import lax

D = 2048
HEADS = 16
HEAD = 128
DC = 2048
CW = 31
BLOCK = 64
TOK_DEV = 1024
DH = 2048
TOKENS = 32768
N_TP = 4


def draw_forget_gap(key, part):
    order = jax.random.permutation(jax.random.fold_in(key, 3), HEADS)
    fast_count = HEADS // 2
    fast = order < fast_count
    spread = jax.random.uniform(jax.random.fold_in(key, 5), (HEADS, HEAD), jnp.float32)
    slow_gap = jnp.exp(jnp.log(0.5) + spread * jnp.log(3.0)) / TOKENS
    fast_gap = jnp.exp(jnp.log(0.03) + spread * jnp.log(10.0 / 3.0))
    return jnp.where(fast[:, None], fast_gap, slow_gap).reshape(HEADS * HEAD)


def draw_decay_shift(key, part):
    block_total = TOKENS // TOK_DEV
    spread = jax.random.uniform(jax.random.fold_in(key, 7), (block_total, 1), jnp.float32)
    rate = jnp.exp(jnp.log(0.2) + spread * jnp.log(5.0)) / TOKENS
    smooth_part = -jnp.repeat(rate, TOK_DEV, axis=0) * jnp.ones((1, HEADS), jnp.float32)
    positions = jax.random.randint(jax.random.fold_in(key, 11), (2,), 0, TOKENS)
    depth = jax.random.uniform(jax.random.fold_in(key, 13), (2, HEADS), jnp.float32, 0.2, 0.4)
    hits = (jnp.arange(TOKENS)[:, None] == positions[None, :]).astype(jnp.float32)
    return smooth_part + jnp.dot(hits, jnp.log(1.0 - depth))


def draw_conv_taps(key, part):
    channel_rise = jnp.exp(jnp.log(3.0) * jnp.arange(DC).astype(jnp.float32) / DC)
    base = jnp.clip(jax.random.normal(jax.random.fold_in(key, 17), (CW, DC), jnp.float32), -4.0, 4.0)
    spread = jnp.exp(jax.random.uniform(jax.random.fold_in(key, 19), (DC,), jnp.float32, 0.0, jnp.log(10.0)))
    scale = 0.1
    return base * channel_rise * spread * scale


def levels(rng, shape, split, least, top_value):
    factor_of = 1.0
    for dim, blocks in split:
        steps = jax.random.uniform(jax.random.fold_in(jax.random.fold_in(rng, 6), dim), (blocks,), jnp.float32, least / len(split), top_value / len(split))
        factor_of = factor_of * jnp.repeat(jnp.exp(steps), shape[dim] // blocks).reshape((-1,) + (1,) * (len(shape) - 1 - dim))
    return factor_of


def gaussian(rng, dims, scale, most, split=(), kind=jnp.bfloat16):
    level = levels(rng, dims, split, -0.22, 0.18) if split else 1.0
    values = jax.random.normal(rng, dims, jnp.float32) * scale * level
    return jnp.minimum(jnp.maximum(values, -most), most).astype(kind)


def setup_inputs(seed: int = 0) -> dict:
    streams_of = jax.random.split(jax.random.key(seed), 16)
    tokens = gaussian(streams_of[0], (TOKENS, D), 1.0, 6.0, ((0, 128),))
    norm_gain = jnp.clip(1.0 + 0.18 * jax.random.normal(streams_of[1], (D,), jnp.float32), 0.1, 1.9)
    w_query = gaussian(streams_of[2], (D, DH), D ** -0.5, 0.125, ((1, 4),))
    w_forget = gaussian(streams_of[3], (D, DH), D ** -0.5, 0.125, ((1, 4),))
    w_value = gaussian(streams_of[4], (D, DH), D ** -0.5, 0.125, ((1, 4),))
    w_rgate = gaussian(streams_of[5], (D, DH), D ** -0.5, 0.125, ((1, 4),))
    w_glu_value = gaussian(streams_of[6], (D, DC), D ** -0.5, 0.125, ((1, 4),))
    w_glu_gate = gaussian(streams_of[7], (D, DC), D ** -0.5, 0.125, ((1, 4),))
    forget_gap = draw_forget_gap(jax.random.fold_in(streams_of[15], 71), 0)
    decay_shift = draw_decay_shift(jax.random.fold_in(streams_of[15], 71), 0)
    head_gain = jnp.clip(1.0 + 0.18 * jax.random.normal(streams_of[10], (HEAD,), jnp.float32), 0.1, 1.9)
    conv_taps = draw_conv_taps(jax.random.fold_in(streams_of[15], 71), 0)
    conv_gain = jnp.clip(1.0 + 0.18 * jax.random.normal(streams_of[12], (DC,), jnp.float32), 0.1, 1.9)
    out_rec = gaussian(streams_of[13], (DH, D), (DH + DC) ** -0.5, 0.09375, ((0, 4),))
    out_conv = gaussian(streams_of[14], (DC, D), (DH + DC) ** -0.5, 0.09375, ((0, 4),))
    return {"tokens": tokens, "norm_gain": norm_gain, "w_query": w_query, "w_forget": w_forget, "w_value": w_value, "w_rgate": w_rgate, "w_glu_value": w_glu_value, "w_glu_gate": w_glu_gate, "forget_gap": forget_gap, "decay_shift": decay_shift, "head_gain": head_gain, "conv_taps": conv_taps, "conv_gain": conv_gain, "out_rec": out_rec, "out_conv": out_conv}


precise_setting = lax.Precision.HIGHEST
norm_epsilon = 1e-05
head_epsilon = 1e-06

def layer_norm(values, gain):
    widened = values.astype(jnp.float32)
    row_mean = lax.optimization_barrier(jnp.mean(widened, axis=-1, keepdims=True))
    centred = widened - row_mean
    row_var = lax.optimization_barrier(jnp.mean(centred * centred, axis=-1, keepdims=True))
    return centred * lax.rsqrt(row_var + norm_epsilon) * gain.astype(jnp.float32)

def block_scan(query, key_gate, values, log_forget):
    row_count, head_count, key_width = query.shape
    value_width = values.shape[2]
    block_count = row_count // BLOCK

    def to_blocks(array):
        return array.reshape(block_count, BLOCK, head_count, array.shape[2]).transpose(0, 2, 1, 3)
    causal = lax.broadcasted_iota(jnp.int32, (BLOCK, BLOCK), 0) >= lax.broadcasted_iota(jnp.int32, (BLOCK, BLOCK), 1)

    def advance(current_state, inputs):
        query_blk, key_block, value_block, log_blk = inputs
        running_total = jnp.cumsum(log_blk, axis=1)
        closing_log = running_total[:, -1:, :]
        query_decayed = query_blk * jnp.exp(running_total)
        scores = jnp.einsum('htk,hsk->hts', query_decayed, key_block * jnp.exp(-running_total), precision=precise_setting)
        scores = jnp.where(causal[None], scores, 0.0)
        output_rows = jnp.einsum('hts,hsv->htv', scores, value_block, precision=precise_setting)
        output_rows = output_rows + jnp.einsum('ori,oiq->orq', query_decayed, current_state, precision=precise_setting)
        current_state = jnp.exp(closing_log[:, 0, :])[:, :, None] * current_state + jnp.einsum('itp,ito->ipo', key_block * jnp.exp(closing_log - running_total), value_block, precision=precise_setting)
        return (current_state, output_rows)
    start_state = jnp.zeros((head_count, key_width, value_width), jnp.float32)
    final_state, output_rows = lax.scan(advance, start_state, (to_blocks(query), to_blocks(key_gate), to_blocks(values), to_blocks(log_forget)))
    return output_rows.transpose(0, 2, 1, 3).reshape(row_count, head_count, value_width)

def reference(tokens, norm_gain, w_query, w_forget, w_value, w_rgate, w_glu_value, w_glu_gate, forget_gap, decay_shift, head_gain, conv_taps, conv_gain, out_rec, out_conv):
    normed = layer_norm(tokens, norm_gain).astype(jnp.bfloat16)

    def project(weight):
        return jnp.dot(normed, weight, preferred_element_type=jnp.float32).astype(jnp.bfloat16)
    query_raw = project(w_query)
    forget_raw = project(w_forget)
    value_raw = project(w_value)
    rgate_raw = project(w_rgate)
    glu_value = project(w_glu_value)
    glu_gate = project(w_glu_gate)
    seq_len = tokens.shape[0]
    query = jax.nn.silu(query_raw.astype(jnp.float32)).reshape(seq_len, HEADS, HEAD)
    key_gate = forget_gap * jax.nn.sigmoid(-forget_raw.astype(jnp.float32))
    log_forget = jnp.log1p(-key_gate).reshape(seq_len, HEADS, HEAD) + decay_shift[:, :, None]
    values = value_raw.astype(jnp.float32).reshape(seq_len, HEADS, HEAD)
    recurrent_branch = block_scan(query, key_gate.reshape(seq_len, HEADS, HEAD), values, log_forget)
    recurrent_branch = recurrent_branch * lax.rsqrt(lax.optimization_barrier(jnp.mean(recurrent_branch * recurrent_branch, axis=-1, keepdims=True)) + head_epsilon) * head_gain
    rec_out = (recurrent_branch.reshape(seq_len, HEADS * HEAD) * jax.nn.silu(rgate_raw.astype(jnp.float32))).astype(jnp.bfloat16)
    mixed_in = (glu_value.astype(jnp.float32) * jax.nn.sigmoid(glu_gate.astype(jnp.float32))).astype(jnp.bfloat16)
    padded = lax.optimization_barrier(jnp.concatenate([jnp.zeros((CW - 1, DC), jnp.bfloat16), mixed_in], axis=0)).astype(jnp.float32)
    filtered = jnp.zeros((seq_len, DC), jnp.float32)
    for tap_index in range(CW):
        filtered = filtered + conv_taps[tap_index] * padded[tap_index:tap_index + seq_len]
    conv_out = jax.nn.silu(layer_norm(filtered, conv_gain)).astype(jnp.bfloat16)
    rec_share = HEADS * HEAD // N_TP
    conv_share = DC // N_TP
    mixed = jnp.zeros((seq_len, D), jnp.float32)
    for group in range(N_TP):
        term = jnp.dot(rec_out[:, group * rec_share:(group + 1) * rec_share], out_rec[group * rec_share:(group + 1) * rec_share], preferred_element_type=jnp.float32)
        term = term + jnp.dot(conv_out[:, group * conv_share:(group + 1) * conv_share], out_conv[group * conv_share:(group + 1) * conv_share], preferred_element_type=jnp.float32)
        mixed = mixed + lax.optimization_barrier(term.astype(jnp.bfloat16)).astype(jnp.float32)
    return mixed.astype(jnp.bfloat16)
```

```python
import functools

import jax
import jax.numpy as jnp
import numpy as np
from jax import lax
from jax.experimental import pallas as pl
from jax.experimental.pallas import tpu as pltpu
from jax.sharding import PartitionSpec as P

HEAD = 128
BLK = 128
NORM_EPS = 1e-05
HEAD_EPS = 1e-06
F32 = jnp.float32
BF16 = jnp.bfloat16


SLOT = np.array([[0, 1], [5, 3], [6, 7], [2, 4]])
SLOT_TABLE = np.array(
    [[SLOT[(p // 2 - t) % 4][p % 2] for p in range(8)] for t in range(4)], dtype=np.int32
)
PLACE_TABLE = np.argsort(SLOT_TABLE, axis=1).astype(np.int32)


def params(**kw):
    return pltpu.CompilerParams(vmem_limit_bytes=58 * 1024 * 1024, **kw)


def dot(a, b, dims=((1,), (0,))):
    return lax.dot_general(a, b, (dims, ((), ())), preferred_element_type=F32)


def silu(x):
    return x * jax.nn.sigmoid(x)


def project_kernel(count, buffers, *refs):
    x0, x1, gain = refs[:3]
    weights = refs[3 : 3 + count]
    refs = refs[3 + count + buffers :]
    outs, (normed, wbuf, sems) = refs[:-3], refs[-3:]
    copies = [pltpu.make_async_copy(weights[n], wbuf.at[n], sems.at[n]) for n in range(count)]
    for copy in copies:
        copy.start()
    g = gain[...]
    for k, x in enumerate((x0, x1)):
        for r in range(0, BLK, 32):
            rows = x[r : r + 32, :].astype(F32)
            centred = rows - jnp.mean(rows, axis=-1, keepdims=True)
            var = jnp.mean(centred * centred, axis=-1, keepdims=True)
            normed[k * BLK + r : k * BLK + r + 32, :] = (
                centred * lax.rsqrt(var + NORM_EPS) * g
            ).astype(BF16)
    done = 0
    for out in outs:
        for n in range(out.shape[1] // 512):
            copies[done].wait()
            out[:, n * 512 : (n + 1) * 512] = dot(normed[...], wbuf[done]).astype(BF16)
            done += 1


def project(group, x0, x1, gain, weights, bufs, widths):
    count, depth = len(weights), x0.shape[1]
    any_spec = pl.BlockSpec(memory_space=pl.ANY)
    fixed = lambda shape: pl.BlockSpec(shape, lambda i: (0, 0))
    aliased = [] if bufs is None else list(bufs)
    return pl.pallas_call(
        functools.partial(project_kernel, count, len(aliased)),
        grid=(1,),
        in_specs=[fixed(x0.shape), fixed(x1.shape), fixed(gain.shape)]
        + [any_spec] * (count + len(aliased)),
        out_specs=[pl.BlockSpec((2 * BLK, w), lambda i: (group, 0)) for w in widths],
        out_shape=[jax.ShapeDtypeStruct((8 * BLK, w), BF16) for w in widths],
        scratch_shapes=[
            pltpu.VMEM((2 * BLK, depth), BF16),
            pltpu.VMEM((count, depth, 512), BF16),
            pltpu.SemaphoreType.DMA((count,)),
        ],
        input_output_aliases={3 + count + k: k for k in range(len(aliased))},
        compiler_params=params(),
        cost_estimate=pl.CostEstimate(
            flops=2 * 2 * BLK * depth * 512 * count, bytes_accessed=count * depth * 1024, transcendentals=0
        ),
        name=f"project_{group}_{count}",
    )(x0, x1, gain, *weights, *aliased)


def gates(forget_ref, gap_ref, shift_ref):
    key = gap_ref[...] * jax.nn.sigmoid(-forget_ref[...].astype(F32))
    shift = shift_ref[...]
    spread = jnp.concatenate(
        [jnp.broadcast_to(shift[:, h : h + 1], (BLK, HEAD)) for h in range(4)], axis=1
    )
    log_forget = jnp.log1p(-key) + spread
    high = log_forget.astype(BF16)
    low = (log_forget - high.astype(F32)).astype(BF16)
    rows = lax.broadcasted_iota(jnp.int32, (BLK, BLK), 0)
    cols = lax.broadcasted_iota(jnp.int32, (BLK, BLK), 1)
    lower = (rows >= cols).astype(F32).astype(BF16)
    return key, dot(lower, high) + dot(lower, low)


def pieces(log_row):
    high = log_row.astype(BF16).astype(F32)
    mid = (log_row - high).astype(BF16).astype(F32)
    low = log_row - high - mid
    row = lax.broadcasted_iota(jnp.int32, (16, HEAD), 0)
    tile = jnp.where(row == 0, high, jnp.where(row == 1, mid, jnp.where(row == 2, low, 0.0)))
    return tile.astype(BF16)


def states_kernel(table, forget, value, shift, gap, pack, starts, offsets, state, offset):
    i = pl.program_id(0)

    @pl.when(i == 0)
    def _():
        state[...] = jnp.zeros_like(state)
        offset[...] = jnp.zeros_like(offset)

    key, run = gates(forget, gap, shift)
    close = run[BLK - 1 : BLK, :]
    key_far = (key * jnp.exp(close - run)).astype(BF16)
    keep = jnp.exp(close)
    offsets[0] = jnp.broadcast_to(offset[0:1, :], (8, 4 * HEAD))
    total = offset[0:1, :] + close
    offset[0:1, :] = total
    for h in range(4):
        lanes = slice(h * HEAD, (h + 1) * HEAD)
        before = state[h]
        starts[0, h] = before.astype(BF16)
        state[h] = before * keep[:, lanes] + dot(value[:, lanes], key_far[:, lanes], ((0,), (0,)))

    @pl.when(i == 7)
    def _():
        for h in range(4):
            pack[h, 0:HEAD, :] = state[h].astype(BF16)
            pack[h, HEAD : HEAD + 16, :] = pieces(total[:, h * HEAD : (h + 1) * HEAD])


def local_states(table, fv, shift, gap):
    return pl.pallas_call(
        states_kernel,
        grid_spec=pltpu.PrefetchScalarGridSpec(
            num_scalar_prefetch=1,
            grid=(8,),
            in_specs=[
                pl.BlockSpec((BLK, 512), lambda i, t: (t[i], 0)),
                pl.BlockSpec((BLK, 512), lambda i, t: (t[i], 1)),
                pl.BlockSpec((BLK, 4), lambda i, t: (i, 0)),
                pl.BlockSpec((1, 512), lambda i, t: (0, 0)),
            ],
            out_specs=[
                pl.BlockSpec((4, HEAD + 16, HEAD), lambda i, t: (0, 0, 0)),
                pl.BlockSpec((1, 4, HEAD, HEAD), lambda i, t: (i, 0, 0, 0)),
                pl.BlockSpec((1, 8, 512), lambda i, t: (i, 0, 0)),
            ],
            scratch_shapes=[pltpu.VMEM((4, HEAD, HEAD), F32), pltpu.VMEM((8, 512), F32)],
        ),
        out_shape=[
            jax.ShapeDtypeStruct((4, HEAD + 16, HEAD), BF16),
            jax.ShapeDtypeStruct((8, 4, HEAD, HEAD), BF16),
            jax.ShapeDtypeStruct((8, 8, 512), F32),
        ],
        compiler_params=params(),
        cost_estimate=pl.CostEstimate(flops=4 * 10**9, bytes_accessed=4 * 2**20, transcendentals=0),
        name="local_states",
    )(table, fv, fv, shift, gap)


def outputs_kernel(table, forget, value, query, shift, gap, starts, offsets, near, distant):
    key, run = gates(forget, gap, shift)
    middle = run[BLK // 2 - 1 : BLK // 2, :]
    query_f = silu(query[...].astype(F32))
    query_mid = query_f * jnp.exp(run - middle)
    key_mid = (key * jnp.exp(middle - run)).astype(BF16)
    query_near = (query_mid * jnp.exp(middle)).astype(BF16)
    distant[...] = (query_mid * jnp.exp(middle + offsets[0, 0:1, :])).astype(BF16)
    query_mid = query_mid.astype(BF16)
    rows = lax.broadcasted_iota(jnp.int32, (BLK, BLK), 0)
    cols = lax.broadcasted_iota(jnp.int32, (BLK, BLK), 1)
    for h in range(4):
        lanes = slice(h * HEAD, (h + 1) * HEAD)
        scores = dot(query_mid[:, lanes], key_mid[:, lanes], ((1,), (1,)))
        scores = jnp.where(rows >= cols, scores, 0.0).astype(BF16)
        near[:, lanes] = dot(scores, value[:, lanes]) + dot(
            query_near[:, lanes], starts[0, h], ((1,), (1,))
        )


def local_outputs(table, fv, qr, shift, gap, starts, offsets):
    return pl.pallas_call(
        outputs_kernel,
        grid_spec=pltpu.PrefetchScalarGridSpec(
            num_scalar_prefetch=1,
            grid=(8,),
            in_specs=[
                pl.BlockSpec((BLK, 512), lambda i, t: (t[i], 0)),
                pl.BlockSpec((BLK, 512), lambda i, t: (t[i], 1)),
                pl.BlockSpec((BLK, 512), lambda i, t: (t[i], 0)),
                pl.BlockSpec((BLK, 4), lambda i, t: (i, 0)),
                pl.BlockSpec((1, 512), lambda i, t: (0, 0)),
                pl.BlockSpec((1, 4, HEAD, HEAD), lambda i, t: (i, 0, 0, 0)),
                pl.BlockSpec((1, 8, 512), lambda i, t: (i, 0, 0)),
            ],
            out_specs=[
                pl.BlockSpec((BLK, 512), lambda i, t: (t[i], 0)),
                pl.BlockSpec((BLK, 512), lambda i, t: (t[i], 0)),
            ],
        ),
        out_shape=[
            jax.ShapeDtypeStruct((8 * BLK, 512), F32),
            jax.ShapeDtypeStruct((8 * BLK, 512), BF16),
        ],
        compiler_params=params(),
        cost_estimate=pl.CostEstimate(flops=6 * 10**9, bytes_accessed=7 * 2**20, transcendentals=0),
        name="local_outputs",
    )(table, fv, fv, qr, shift, gap, starts, offsets)


def unpack(ref, h):
    tile = ref[h, HEAD : HEAD + 16, :].astype(F32)
    return ref[h, 0:HEAD, :].astype(F32), tile[0:1] + tile[1:2] + tile[2:3]


def ordered_pair(core, mine, other, h):
    (mine_s, mine_l), (other_s, other_l) = unpack(mine, h), unpack(other, h)
    lead = core == 0
    first = (jnp.where(lead, mine_s, other_s), jnp.where(lead, mine_l, other_l))
    second = (jnp.where(lead, other_s, mine_s), jnp.where(lead, other_l, mine_l))
    return first, second


def chip_kernel(where, mine, other, total):
    for h in range(2):
        (s0, l0), (s1, l1) = ordered_pair(where[0], mine, other, h)
        total[h, 0:HEAD, :] = (jnp.exp(l1) * s0 + s1).astype(BF16)
        total[h, HEAD : HEAD + 16, :] = pieces(l0 + l1)


def row_kernel(where, own, back1, back2, back3, total, before, before_log):
    y = where[1]
    for h in range(2):
        parts = [unpack(ref, h) for ref in (own, back1, back2, back3)]
        place = [lax.rem(y + 4 - d, 4) for d in range(4)]
        sum_s, sum_l = jnp.zeros((HEAD, HEAD), F32), jnp.zeros((1, HEAD), F32)
        pre_s, pre_l = jnp.zeros((HEAD, HEAD), F32), jnp.zeros((1, HEAD), F32)
        for d in range(4):
            later = jnp.zeros((1, HEAD), F32)
            for e in range(4):
                if e != d:
                    later = later + jnp.where(place[e] > place[d], parts[e][1], 0.0)
            sum_s = sum_s + jnp.exp(later) * parts[d][0]
            sum_l = sum_l + parts[d][1]
            if d:
                behind = y >= d
                pre_s = pre_s + jnp.where(behind, jnp.exp(pre_l), 0.0) * parts[d][0]
                pre_l = pre_l + jnp.where(behind, parts[d][1], 0.0)
        total[h, 0:HEAD, :] = sum_s.astype(BF16)
        total[h, HEAD : HEAD + 16, :] = pieces(sum_l)
        before[h] = pre_s
        before_log[h] = jnp.broadcast_to(pre_l, (8, HEAD))


def arriving_kernel(where, mine, other, before, before_log, back1, back2, back3, keep, send):
    core = where[0]
    for h in range(2):
        state, log = jnp.zeros((HEAD, HEAD), F32), jnp.zeros((1, HEAD), F32)
        for ref in (back1, back2, back3):
            s, l = unpack(ref, h)
            state = state + jnp.exp(log) * s
            log = log + l
        state = jnp.exp(before_log[h, 0:1, :]) * state + before[h]
        (s0, l0), _ = ordered_pair(core, mine, other, h)
        later = jnp.exp(l0) * state + s0
        keep[h] = jnp.where(core == 0, state, later).astype(BF16)
        send[h] = jnp.where(core == 0, later, state).astype(BF16)


def small(kernel, where, args, shapes, name):
    whole = [pl.BlockSpec(memory_space=pltpu.VMEM) for _ in args]
    return pl.pallas_call(
        kernel,
        in_specs=[pl.BlockSpec(memory_space=pltpu.SMEM)] + whole,
        out_specs=[pl.BlockSpec(memory_space=pltpu.VMEM) for _ in shapes],
        out_shape=[jax.ShapeDtypeStruct(s, d) for s, d in shapes],
        compiler_params=params(),
        cost_estimate=pl.CostEstimate(flops=10**8, bytes_accessed=2**20, transcendentals=0),
        name=name,
    )(where, *args)


def arriving_states(pack, where):
    core = where[0]
    tall = (2, HEAD + 16, HEAD)
    mine = lax.dynamic_slice_in_dim(pack, 2 * core, 2, 0)
    theirs = lax.dynamic_slice_in_dim(pack, 2 - 2 * core, 2, 0)
    swap = [(i, i ^ 1) for i in range(32)]
    other = lax.ppermute(theirs, "sp", swap)
    (total,) = small(chip_kernel, where, (mine, other), [(tall, BF16)], "chip_total")
    rows = [
        lax.ppermute(total, "sp", [(i, i // 8 * 8 + (i + 2 * d) % 8) for i in range(32)])
        for d in (1, 2, 3)
    ]
    slab, before, before_log = small(
        row_kernel,
        where,
        (total, *rows),
        [(tall, BF16), ((2, HEAD, HEAD), F32), ((2, 8, HEAD), F32)],
        "row_total",
    )
    slabs = [
        lax.ppermute(slab, "sp", [(i, i + 8 * d) for i in range(32 - 8 * d)]) for d in (1, 2, 3)
    ]
    half = ((2, HEAD, HEAD), BF16)
    keep, send = small(
        arriving_kernel, where, (mine, other, before, before_log, *slabs), [half, half], "arriving"
    )
    return keep, lax.ppermute(send, "sp", swap)


def filter_kernel(table, value, gate, halo, taps, filtered, stats, window):
    i = pl.program_id(0)
    reach = 32

    def mix(v, g):
        return (v.astype(F32) * jax.nn.sigmoid(g.astype(F32))).astype(BF16).astype(F32)

    @pl.when(i == 0)
    def _():
        window[0:reach, :] = mix(halo[:, 0:512], halo[:, 512:1024])

    @pl.when(i > 0)
    def _():
        window[0:reach, :] = window[BLK : BLK + reach, :]

    window[reach : reach + BLK, :] = mix(value[...], gate[...])
    row_sum = jnp.zeros((BLK, HEAD), F32)
    row_square = jnp.zeros((BLK, HEAD), F32)
    for c in range(4):
        lanes = slice(c * HEAD, (c + 1) * HEAD)
        acc = jnp.zeros((BLK, HEAD), F32)
        for j in range(31):
            acc = acc + taps[j : j + 1, lanes] * window[2 + j : 2 + j + BLK, lanes]
        filtered[:, lanes] = acc
        row_sum = row_sum + acc
        row_square = row_square + acc * acc
    lane = lax.broadcasted_iota(jnp.int32, (BLK, HEAD), 1)
    tile = jnp.where(
        lane == 0,
        jnp.sum(row_sum, axis=1, keepdims=True),
        jnp.where(lane == 1, jnp.sum(row_square, axis=1, keepdims=True), 0.0),
    )
    stats[...] = jnp.transpose(tile)[0:8, :]


def filter_rows(table, qr, halo, taps):
    return pl.pallas_call(
        filter_kernel,
        grid_spec=pltpu.PrefetchScalarGridSpec(
            num_scalar_prefetch=1,
            grid=(8,),
            in_specs=[
                pl.BlockSpec((BLK, 512), lambda i, t: (t[i], 2)),
                pl.BlockSpec((BLK, 512), lambda i, t: (t[i], 3)),
                pl.BlockSpec((32, 1024), lambda i, t: (0, 0)),
                pl.BlockSpec((31, 512), lambda i, t: (0, 0)),
            ],
            out_specs=[
                pl.BlockSpec((BLK, 512), lambda i, t: (t[i], 0)),
                pl.BlockSpec((8, BLK), lambda i, t: (0, i)),
            ],
            scratch_shapes=[pltpu.VMEM((32 + BLK, 512), F32)],
        ),
        out_shape=[
            jax.ShapeDtypeStruct((8 * BLK, 512), F32),
            jax.ShapeDtypeStruct((8, 8 * BLK), F32),
        ],
        compiler_params=params(),
        cost_estimate=pl.CostEstimate(flops=9 * 10**9, bytes_accessed=5 * 2**20, transcendentals=0),
        name="filter_rows",
    )(table, qr, qr, halo, taps)


def merge_kernel(group, added, where, *refs):
    near, distant, rgate, keep, recv, head_gain, filtered, s0, s1, s2, s3, conv_gain, w_rec, w_conv = refs[:14]
    addends = refs[14 : 14 + added]
    top, bottom, act = refs[14 + added :]

    @pl.when(pl.program_id(0) == 0)
    def _():
        for h in range(4):
            lanes = slice(h * HEAD, (h + 1) * HEAD)
            k = h % 2
            state = jnp.where(where[0] == h // 2, keep[k].astype(F32), recv[k].astype(F32)).astype(BF16)
            rec = near[:, lanes] + dot(distant[:, lanes], state, ((1,), (1,)))
            rec = rec * lax.rsqrt(jnp.mean(rec * rec, axis=-1, keepdims=True) + HEAD_EPS)
            rec = rec * head_gain[...] * silu(rgate[:, lanes].astype(F32))
            act[:, lanes] = rec.astype(BF16)
        for k in range(2):
            rows = slice(k * BLK, (k + 1) * BLK)
            at = pl.ds(pl.multiple_of(where[2 + 2 * group + k] * BLK, BLK), BLK)
            stats = (s0[:, at] + s1[:, at]) + (s2[:, at] + s3[:, at])
            tile = jnp.transpose(jnp.concatenate([stats] * 16, axis=0))
            mean = tile[:, 0:1] / 2048.0
            scale = lax.rsqrt(tile[:, 1:2] / 2048.0 - mean * mean + NORM_EPS)
            normed = (filtered[rows, :] - mean) * scale * conv_gain[...]
            act[rows, 512:1024] = silu(normed).astype(BF16)

    part = dot(act[:, 0:512], w_rec[...]) + dot(act[:, 512:1024], w_conv[...])
    for k, out in enumerate((top, bottom)):
        piece = part[k * BLK : (k + 1) * BLK, :]
        if added:
            piece = piece + addends[k][...].astype(F32)
        out[...] = piece.astype(BF16)


def merge(group, where, near, distant, qr, keep, recv, head_gain, filtered, stats, conv_gain, out_rec, out_conv, addends=()):
    rows = 2 * BLK
    pair = pl.BlockSpec((BLK, 512), lambda n: (0, n))
    return pl.pallas_call(
        functools.partial(merge_kernel, group, len(addends)),
        grid=(4,),
        in_specs=[
            pl.BlockSpec(memory_space=pltpu.SMEM),
            pl.BlockSpec((rows, 512), lambda n: (group, 0)),
            pl.BlockSpec((rows, 512), lambda n: (group, 0)),
            pl.BlockSpec((rows, 512), lambda n: (group, 1)),
            pl.BlockSpec((2, HEAD, HEAD), lambda n: (0, 0, 0)),
            pl.BlockSpec((2, HEAD, HEAD), lambda n: (0, 0, 0)),
            pl.BlockSpec((1, HEAD), lambda n: (0, 0)),
            pl.BlockSpec((rows, 512), lambda n: (group, 0)),
        ]
        + [pl.BlockSpec((8, 8 * BLK), lambda n: (0, 0))] * 4
        + [
            pl.BlockSpec((1, 512), lambda n: (0, 0)),
            pl.BlockSpec((512, 512), lambda n: (0, n)),
            pl.BlockSpec((512, 512), lambda n: (0, n)),
        ]
        + [pair] * len(addends),
        out_specs=[pair, pair],
        out_shape=[jax.ShapeDtypeStruct((BLK, 2048), BF16)] * 2,
        scratch_shapes=[pltpu.VMEM((rows, 1024), BF16)],
        compiler_params=params(),
        cost_estimate=pl.CostEstimate(
            flops=2 * rows * 1024 * 2048, bytes_accessed=7 * 2**20, transcendentals=0
        ),
        name=f"merge_{group}",
    )(where, near, distant, qr, keep, recv, head_gain, filtered, *stats, conv_gain, out_rec, out_conv, *addends)


def on_device(
    tokens,
    norm_gain,
    w_query,
    w_forget,
    w_value,
    w_rgate,
    w_glu_value,
    w_glu_gate,
    forget_gap,
    decay_shift,
    head_gain,
    conv_taps,
    conv_gain,
    out_rec,
    out_conv,
):
    along = functools.partial(lax.ppermute, axis_name="tp")
    ahead = [(i, (i + 1) % 4) for i in range(4)]
    behind = [(i, (i - 1) % 4) for i in range(4)]
    t, s = lax.axis_index("tp"), lax.axis_index("sp")
    table = lax.dynamic_index_in_dim(jnp.asarray(SLOT_TABLE), t, 0, keepdims=False)
    place = lax.dynamic_index_in_dim(jnp.asarray(PLACE_TABLE), t, 0, keepdims=False)
    where = jnp.concatenate([jnp.stack([s % 2, (s // 2) % 4]).astype(jnp.int32), place])

    a, b = tokens[:BLK], tokens[BLK:]
    from_back_a = along(a, perm=ahead)
    from_front_b = along(b, perm=behind)
    from_back_b = along(b, perm=ahead)
    from_front_a = along(a, perm=behind)
    far_a = along(from_back_a, perm=ahead)
    far_b = along(from_front_b, perm=behind)

    gain = norm_gain[None, :]
    gap = forget_gap[None, :]
    first, rest = (w_forget, w_value), (w_query, w_rgate, w_glu_value, w_glu_gate)
    bufs = project(0, a, b, gain, first + rest, None, (1024, 2048))
    bufs = project(1, from_back_a, from_front_b, gain, first + rest, bufs, (1024, 2048))
    fv, qr = project(2, from_back_b, from_front_a, gain, first + rest, bufs, (1024, 2048))
    (fv,) = project(3, far_a, far_b, gain, first, (fv,), (1024,))
    pack, starts, offsets = local_states(table, fv, decay_shift, gap)
    keep, recv = arriving_states(pack, where)
    (qr,) = project(3, far_a, far_b, gain, rest, (qr,), (2048,))

    edge = lax.dynamic_slice(qr, (table[7] * BLK + BLK - 32, 1024), (32, 1024))
    halo = lax.ppermute(edge, "sp", [(i, i + 1) for i in range(31)])
    filtered, stats = filter_rows(table, qr, halo, conv_taps)
    near, distant = local_outputs(table, fv, qr, decay_shift, gap, starts, offsets)
    stats_all = [stats] + [along(stats, perm=[(i, (i + d) % 4) for i in range(4)]) for d in (1, 2, 3)]

    common = (where, near, distant, qr, keep, recv, head_gain[None, :], filtered, stats_all, conv_gain[None, :], out_rec, out_conv)
    far_top, far_bottom = merge(3, *common)
    via_back = along(far_top, perm=ahead)
    via_front = along(far_bottom, perm=behind)
    back_a, front_b = merge(1, *common)
    got_b = along(front_b, perm=ahead)
    got_a = along(back_a, perm=behind)
    back_b, front_a = merge(2, *common, addends=(via_front, via_back))
    sum_a = along(front_a, perm=ahead)
    sum_b = along(back_b, perm=behind)
    own_a, own_b = merge(0, *common)
    total = lambda *parts: functools.reduce(jnp.add, [p.astype(F32) for p in parts]).astype(BF16)
    return jnp.concatenate([total(own_a, got_a, sum_a), total(own_b, got_b, sum_b)], axis=0)


def solution(mesh):
    placed = (
        P(("sp", "tp"), None),
        P(),
        P(None, "tp"),
        P(None, "tp"),
        P(None, "tp"),
        P(None, "tp"),
        P(None, "tp"),
        P(None, "tp"),
        P("tp"),
        P("sp", "tp"),
        P(),
        P(None, "tp"),
        P("tp"),
        P("tp", None),
        P("tp", None),
    )
    return jax.shard_map(
        on_device, mesh=mesh, in_specs=placed, out_specs=P(("sp", "tp"), None), check_vma=False
    )
```

```python
import functools

import jax
import jax.numpy as jnp
import numpy as np
from jax import lax
from jax.experimental import pallas as pl
from jax.experimental.pallas import tpu as pltpu
from jax.sharding import PartitionSpec as P


HEAD = 128
BLK = 128
NORM_EPS = 1e-05
HEAD_EPS = 1e-06
F32 = jnp.float32
BF16 = jnp.bfloat16


SLOT = np.array([[0, 1], [5, 3], [6, 7], [2, 4]])
SLOT_TABLE = np.array(
    [[SLOT[(p // 2 - t) % 4][p % 2] for p in range(8)] for t in range(4)], dtype=np.int32
)
PLACE_TABLE = np.argsort(SLOT_TABLE, axis=1).astype(np.int32)


def params(**kw):
    return pltpu.CompilerParams(vmem_limit_bytes=58 * 1024 * 1024, **kw)


def dot(a, b, dims=((1,), (0,))):
    return lax.dot_general(a, b, (dims, ((), ())), preferred_element_type=F32)


def silu(x):
    return x * jax.nn.sigmoid(x)


WIDE = 4 * HEAD


def gates(forget, gap, shift):
    key = gap * jax.nn.sigmoid(-forget.astype(F32))
    spread = jnp.concatenate(
        [jnp.broadcast_to(shift[:, h : h + 1], (BLK, HEAD)) for h in range(4)], axis=1
    )
    log_forget = jnp.log1p(-key) + spread
    high = log_forget.astype(BF16)
    low = (log_forget - high.astype(F32)).astype(BF16)
    rows = lax.broadcasted_iota(jnp.int32, (BLK, BLK), 0)
    cols = lax.broadcasted_iota(jnp.int32, (BLK, BLK), 1)
    lower = (rows >= cols).astype(F32).astype(BF16)
    return key, dot(lower, high) + dot(lower, low)


def pieces(log_row):
    high = log_row.astype(BF16).astype(F32)
    mid = (log_row - high).astype(BF16).astype(F32)
    low = log_row - high - mid
    row = lax.broadcasted_iota(jnp.int32, (16, HEAD), 0)
    tile = jnp.where(row == 0, high, jnp.where(row == 1, mid, jnp.where(row == 2, low, 0.0)))
    return tile.astype(BF16)


def block_state(key, run, value, store, close_store):
    close = run[BLK - 1 : BLK, :]
    key_far = (key * jnp.exp(close - run)).astype(BF16)
    close_store(jnp.broadcast_to(close, (8, WIDE)))
    for h in range(4):
        lanes = slice(h * HEAD, (h + 1) * HEAD)
        store(h, dot(value[:, lanes], key_far[:, lanes], ((0,), (0,))))


def block_outputs(key, run, value, query, near, query_near, at):
    middle = run[BLK // 2 - 1 : BLK // 2, :]
    query_mid = silu(query.astype(F32)) * jnp.exp(run - middle)
    key_mid = (key * jnp.exp(middle - run)).astype(BF16)
    query_near[at, :] = (query_mid * jnp.exp(middle)).astype(BF16)
    query_mid = query_mid.astype(BF16)
    rows = lax.broadcasted_iota(jnp.int32, (BLK, BLK), 0)
    cols = lax.broadcasted_iota(jnp.int32, (BLK, BLK), 1)
    for h in range(4):
        lanes = slice(h * HEAD, (h + 1) * HEAD)
        scores = dot(query_mid[:, lanes], key_mid[:, lanes], ((1,), (1,)))
        scores = jnp.where(rows >= cols, scores, 0.0).astype(BF16)
        near[at, lanes] = dot(scores, value[:, lanes])


def fetch(tokens, weights, xbuf, wbuf, sems):
    loads = [
        pltpu.make_async_copy(x, xbuf.at[pl.ds(k * BLK, BLK)], sems.at[k]) for k, x in enumerate(tokens)
    ]
    brings = [
        pltpu.make_async_copy(w, wbuf.at[k], sems.at[len(tokens) + k]) for k, w in enumerate(weights)
    ]
    for copy in loads + brings:
        copy.start()
    return loads, brings


def normalise(loads, xbuf, gain, normed):
    g = gain[...]
    for k, load in enumerate(loads):
        load.wait()
        for r in range(k * BLK, (k + 1) * BLK, 32):
            rows = xbuf[r : r + 32, :].astype(F32)
            centred = rows - jnp.mean(rows, axis=-1, keepdims=True)
            var = jnp.mean(centred * centred, axis=-1, keepdims=True)
            normed[r : r + 32, :] = (centred * lax.rsqrt(var + NORM_EPS) * g).astype(BF16)


def glu(value, gate):
    return (value.astype(F32) * jax.nn.sigmoid(gate.astype(F32))).astype(BF16)


def whole_kernel(slots, aliased, place, *refs):
    tokens, refs = refs[:slots], refs[slots:]
    gain, gap, refs = refs[0], refs[1], refs[2:]
    shifts, refs = refs[:slots], refs[slots:]
    weights, refs = refs[:6], refs[6 + aliased :]
    near, query_near, rgate, mixed, added, close, xbuf, normed, wbuf, raw, sems = refs
    loads, brings = fetch(tokens, weights, xbuf, wbuf, sems)
    normalise(loads, xbuf, gain, normed)

    def times(n):
        brings[n].wait()
        return dot(normed[...], wbuf[n]).astype(BF16)

    for n in range(3):
        raw[n] = times(n)
    for k in range(slots):
        at = slice(k * BLK, (k + 1) * BLK)
        key, run = gates(raw[0, at, :], gap[...], shifts[k][...])
        value = raw[1, at, :]

        def store(h, x):
            added[k, h] = x

        def close_store(x):
            close[k] = x

        block_state(key, run, value, store, close_store)
        block_outputs(key, run, value, raw[2, at, :], near, query_near, at)
    rgate[...] = times(3)
    raw[0] = times(4)
    raw[1] = times(5)
    mixed[...] = glu(raw[0], raw[1])


def any_spec():
    return pl.BlockSpec(memory_space=pl.ANY)


def row_spec(shape):
    return pl.BlockSpec(shape, lambda i, p: (0, 0))


BUFFERS = [((WIDE,), F32), ((WIDE,), BF16), ((WIDE,), BF16), ((WIDE,), BF16)]


def project_whole(first, tokens, place, gain, gap, shift, weights, bufs):
    slots = len(tokens)
    group = first // slots
    depth = tokens[0].shape[1]
    aliased = list(bufs) if bufs is not None else []
    rows = slots * BLK
    flat = lambda: pl.BlockSpec((rows, WIDE), lambda i, p: (group, 0))
    head_inputs = 1 + slots + 2 + slots + 6
    return pl.pallas_call(
        functools.partial(whole_kernel, slots, len(aliased)),
        grid_spec=pltpu.PrefetchScalarGridSpec(
            num_scalar_prefetch=1,
            grid=(1,),
            in_specs=[any_spec()] * slots
            + [row_spec((1, depth)), row_spec((1, WIDE))]
            + [pl.BlockSpec((BLK, 4), lambda i, p, k=k: (p[first + k], 0)) for k in range(slots)]
            + [any_spec()] * (6 + len(aliased)),
            out_specs=[flat(), flat(), flat(), flat()]
            + [
                pl.BlockSpec((slots, 4, HEAD, HEAD), lambda i, p: (group, 0, 0, 0)),
                pl.BlockSpec((slots, 8, WIDE), lambda i, p: (group, 0, 0)),
            ],
            scratch_shapes=[
                pltpu.VMEM((rows, depth), BF16),
                pltpu.VMEM((rows, depth), BF16),
                pltpu.VMEM((6, depth, WIDE), BF16),
                pltpu.VMEM((3, rows, WIDE), BF16),
                pltpu.SemaphoreType.DMA((slots + 6,)),
            ],
        ),
        out_shape=[jax.ShapeDtypeStruct((8 * BLK, *tail), kind) for tail, kind in BUFFERS]
        + [
            jax.ShapeDtypeStruct((8, 4, HEAD, HEAD), F32),
            jax.ShapeDtypeStruct((8, 8, WIDE), F32),
        ],
        input_output_aliases={head_inputs + k: k for k in range(len(aliased))},
        compiler_params=params(),
        cost_estimate=pl.CostEstimate(
            flops=2 * rows * depth * WIDE * 9, bytes_accessed=16 * 2**20, transcendentals=0
        ),
    )(place, *tokens, gain, gap, *[shift] * slots, *weights, *aliased)


def last_states_kernel(place, tokens_a, tokens_b, gain, gap, shift_a, shift_b, w_forget, w_value, added, close, fv, pack, starts, offsets, xbuf, normed, wbuf, parts, sems, more):
    loads, brings = fetch((tokens_a, tokens_b), (w_forget, w_value), xbuf, wbuf, sems)
    bring_parts = pltpu.make_async_copy(added.at[pl.ds(0, 6)], parts.at[pl.ds(0, 6)], more.at[0])
    bring_parts.start()
    normalise(loads, xbuf, gain, normed)
    for n in range(2):
        brings[n].wait()
        fv[:, n * WIDE : (n + 1) * WIDE] = dot(normed[...], wbuf[n]).astype(BF16)
    ends = [None] * 2
    for k, shift in enumerate((shift_a, shift_b)):
        at = slice(k * BLK, (k + 1) * BLK)
        key, run = gates(fv[at, 0:WIDE], gap[...], shift[...])

        def store(h, x):
            parts[6 + k, h] = x

        def close_store(x):
            close_now[k] = x

        close_now = {}
        block_state(key, run, fv[at, WIDE : 2 * WIDE], store, close_store)
        ends[k] = close_now[k]
    bring_parts.wait()
    state = [jnp.zeros((HEAD, HEAD), F32) for _ in range(4)]
    total = jnp.zeros((1, WIDE), F32)
    for i in range(8):
        slot = place[8 + i]
        offsets[slot] = jnp.broadcast_to(total, (8, WIDE))
        end = jnp.where(
            slot == 6, ends[0], jnp.where(slot == 7, ends[1], close[jnp.minimum(slot, 5)])
        )[0:1, :]
        keep = jnp.exp(end)
        for h in range(4):
            lanes = slice(h * HEAD, (h + 1) * HEAD)
            starts[slot, h] = state[h].astype(BF16)
            state[h] = state[h] * keep[:, lanes] + parts[slot, h]
        total = total + end
    for h in range(4):
        tile = pieces(total[:, h * HEAD : (h + 1) * HEAD])
        rows = state[h].astype(BF16)
        for j in range(8):
            pack[8 * h + j, 0:16, :] = rows[16 * j : 16 * j + 16, :]
            pack[8 * h + j, 16:32, :] = tile


def last_states(tokens, place, gain, gap, shift, weights, added, close):
    depth = tokens[0].shape[1]
    rows = 2 * BLK
    return pl.pallas_call(
        last_states_kernel,
        grid_spec=pltpu.PrefetchScalarGridSpec(
            num_scalar_prefetch=1,
            grid=(1,),
            in_specs=[any_spec()] * 2
            + [row_spec((1, depth)), row_spec((1, WIDE))]
            + [pl.BlockSpec((BLK, 4), lambda i, p, k=k: (p[6 + k], 0)) for k in range(2)]
            + [any_spec()] * 3
            + [pl.BlockSpec((8, 8, WIDE), lambda i, p: (0, 0, 0))],
            out_specs=[
                pl.BlockSpec((rows, 2 * WIDE), lambda i, p: (0, 0)),
                pl.BlockSpec((32, 32, HEAD), lambda i, p: (0, 0, 0)),
                pl.BlockSpec((8, 4, HEAD, HEAD), lambda i, p: (0, 0, 0, 0)),
                pl.BlockSpec((8, 8, WIDE), lambda i, p: (0, 0, 0)),
            ],
            scratch_shapes=[
                pltpu.VMEM((rows, depth), BF16),
                pltpu.VMEM((rows, depth), BF16),
                pltpu.VMEM((2, depth, WIDE), BF16),
                pltpu.VMEM((8, 4, HEAD, HEAD), F32),
                pltpu.SemaphoreType.DMA((4,)),
                pltpu.SemaphoreType.DMA((1,)),
            ],
        ),
        out_shape=[
            jax.ShapeDtypeStruct((rows, 2 * WIDE), BF16),
            jax.ShapeDtypeStruct((32, 32, HEAD), BF16),
            jax.ShapeDtypeStruct((8, 4, HEAD, HEAD), BF16),
            jax.ShapeDtypeStruct((8, 8, WIDE), F32),
        ],
        compiler_params=params(),
        cost_estimate=pl.CostEstimate(
            flops=2 * rows * depth * WIDE * 6, bytes_accessed=10 * 2**20, transcendentals=0
        ),
        name="last_states",
    )(place, *tokens, gain, gap, shift, shift, *weights, added, close)


def last_rest_kernel(place, tokens_a, tokens_b, gain, gap, shift_a, shift_b, fv, w_query, w_rgate, w_glu_value, w_glu_gate, b0, b1, b2, b3, near, query_near, rgate, mixed, xbuf, normed, wbuf, raw, sems):
    loads, brings = fetch(
        (tokens_a, tokens_b), (w_glu_value, w_glu_gate, w_query, w_rgate), xbuf, wbuf, sems
    )
    normalise(loads, xbuf, gain, normed)

    def times(n):
        brings[n].wait()
        return dot(normed[...], wbuf[n]).astype(BF16)

    for n in range(3):
        raw[n] = times(n)
    mixed[...] = glu(raw[0], raw[1])
    for k, shift in enumerate((shift_a, shift_b)):
        at = slice(k * BLK, (k + 1) * BLK)
        key, run = gates(fv[at, 0:WIDE], gap[...], shift[...])
        block_outputs(key, run, fv[at, WIDE : 2 * WIDE], raw[2, at, :], near, query_near, at)
    rgate[...] = times(3)


def last_rest(tokens, place, gain, gap, shift, fv, weights, bufs):
    depth = tokens[0].shape[1]
    rows = 2 * BLK
    flat = lambda: pl.BlockSpec((rows, WIDE), lambda i, p: (3, 0))
    return pl.pallas_call(
        last_rest_kernel,
        grid_spec=pltpu.PrefetchScalarGridSpec(
            num_scalar_prefetch=1,
            grid=(1,),
            in_specs=[any_spec()] * 2
            + [row_spec((1, depth)), row_spec((1, WIDE))]
            + [pl.BlockSpec((BLK, 4), lambda i, p, k=k: (p[6 + k], 0)) for k in range(2)]
            + [row_spec((rows, 2 * WIDE))]
            + [any_spec()] * 8,
            out_specs=[flat(), flat(), flat(), flat()],
            scratch_shapes=[
                pltpu.VMEM((rows, depth), BF16),
                pltpu.VMEM((rows, depth), BF16),
                pltpu.VMEM((4, depth, WIDE), BF16),
                pltpu.VMEM((3, rows, WIDE), BF16),
                pltpu.SemaphoreType.DMA((6,)),
            ],
        ),
        out_shape=[jax.ShapeDtypeStruct((8 * BLK, *tail), kind) for tail, kind in BUFFERS],
        input_output_aliases={12 + k: k for k in range(4)},
        compiler_params=params(),
        cost_estimate=pl.CostEstimate(
            flops=2 * rows * depth * WIDE * 6, bytes_accessed=12 * 2**20, transcendentals=0
        ),
        name="last_rest",
    )(place, *tokens, gain, gap, shift, shift, fv, *weights, *bufs)


def prefix_kernel(packs, arriving):
    state = jnp.zeros((16, HEAD), F32)
    for i in range(32):
        arriving[i] = state.astype(BF16)
        tile = packs[i, 16:32, :].astype(F32)
        log = tile[0:1] + tile[1:2] + tile[2:3]
        state = jnp.exp(log) * state + packs[i, 0:16, :].astype(F32)


def arriving_states(pack):
    packs = lax.all_to_all(pack, "sp", split_axis=0, concat_axis=0, tiled=True)
    arriving = pl.pallas_call(
        prefix_kernel,
        out_shape=jax.ShapeDtypeStruct((32, 16, HEAD), BF16),
        compiler_params=params(),
        cost_estimate=pl.CostEstimate(flops=10**8, bytes_accessed=2**20, transcendentals=0),
        name="prefix",
    )(packs)
    arrived = lax.all_to_all(arriving, "sp", split_axis=0, concat_axis=0, tiled=True)
    return arrived.reshape(4, HEAD, HEAD)


def filter_kernel(table, mixed, halo, taps, filtered, stats, window):
    i = pl.program_id(0)
    reach = 32

    @pl.when(i == 0)
    def _():
        window[0:reach, :] = halo[...].astype(F32)

    @pl.when(i > 0)
    def _():
        window[0:reach, :] = window[BLK : BLK + reach, :]

    window[reach : reach + BLK, :] = mixed[...].astype(F32)
    row_sum = jnp.zeros((BLK, HEAD), F32)
    row_square = jnp.zeros((BLK, HEAD), F32)
    for c in range(4):
        lanes = slice(c * HEAD, (c + 1) * HEAD)
        acc = jnp.zeros((BLK, HEAD), F32)
        for r in range(8):
            used = [q for q in range(5) if 0 <= 8 * q + r - 2 < 31]
            shifted = window[8 * used[0] + r : 8 * used[-1] + r + BLK, lanes]
            for q in used:
                j, lead = 8 * q + r - 2, 8 * (q - used[0])
                acc = acc + taps[j : j + 1, lanes] * shifted[lead : lead + BLK, :]
        filtered[:, lanes] = acc
        row_sum = row_sum + acc
        row_square = row_square + acc * acc
    lane = lax.broadcasted_iota(jnp.int32, (BLK, HEAD), 1)
    tile = jnp.where(
        lane == 0,
        jnp.sum(row_sum, axis=1, keepdims=True),
        jnp.where(lane == 1, jnp.sum(row_square, axis=1, keepdims=True), 0.0),
    )
    stats[...] = jnp.transpose(tile)[0:8, :]


def filter_rows(place, mixed, halo, taps):
    return pl.pallas_call(
        filter_kernel,
        grid_spec=pltpu.PrefetchScalarGridSpec(
            num_scalar_prefetch=1,
            grid=(8,),
            in_specs=[
                pl.BlockSpec((BLK, WIDE), lambda i, p: (p[8 + i], 0)),
                pl.BlockSpec((32, WIDE), lambda i, p: (0, 0)),
                pl.BlockSpec((31, WIDE), lambda i, p: (0, 0)),
            ],
            out_specs=[
                pl.BlockSpec((BLK, WIDE), lambda i, p: (p[8 + i], 0)),
                pl.BlockSpec((8, BLK), lambda i, p: (0, i)),
            ],
            scratch_shapes=[pltpu.VMEM((32 + BLK, WIDE), F32)],
        ),
        out_shape=[
            jax.ShapeDtypeStruct((8 * BLK, WIDE), F32),
            jax.ShapeDtypeStruct((8, 8 * BLK), F32),
        ],
        compiler_params=params(),
        cost_estimate=pl.CostEstimate(flops=7 * 10**9, bytes_accessed=5 * 2**20, transcendentals=0),
        name="filter_rows",
    )(place, mixed, halo, taps)


def merge_kernel(group, place, near, query_near, rgate, starts, offsets, arrived, head_gain, filtered, s0, s1, s2, s3, conv_gain, w_rec, w_conv, top, bottom, act):
    @pl.when(pl.program_id(0) == 0)
    def _():
        for k in range(2):
            rows = slice(k * BLK, (k + 1) * BLK)
            carry = jnp.exp(offsets[k, 0:1, :])
            for h in range(4):
                lanes = slice(h * HEAD, (h + 1) * HEAD)
                state = starts[k, h].astype(F32) + carry[:, lanes] * arrived[h].astype(F32)
                rec = near[rows, lanes] + dot(query_near[rows, lanes], state.astype(BF16), ((1,), (1,)))
                rec = rec * lax.rsqrt(jnp.mean(rec * rec, axis=-1, keepdims=True) + HEAD_EPS)
                rec = rec * head_gain[...] * silu(rgate[rows, lanes].astype(F32))
                act[rows, lanes] = rec.astype(BF16)
            at = pl.ds(pl.multiple_of(place[2 * group + k] * BLK, BLK), BLK)
            stats = (s0[:, at] + s1[:, at]) + (s2[:, at] + s3[:, at])
            tile = jnp.transpose(jnp.concatenate([stats] * 16, axis=0))
            mean = tile[:, 0:1] / 2048.0
            scale = lax.rsqrt(tile[:, 1:2] / 2048.0 - mean * mean + NORM_EPS)
            normed = (filtered[rows, :] - mean) * scale * conv_gain[...]
            act[rows, WIDE : 2 * WIDE] = silu(normed).astype(BF16)

    part = dot(act[:, 0:WIDE], w_rec[...]) + dot(act[:, WIDE : 2 * WIDE], w_conv[...])
    top[...] = part[0:BLK, :].astype(BF16)
    bottom[...] = part[BLK : 2 * BLK, :].astype(BF16)


def merge(group, place, near, query_near, rgate, starts, offsets, arrived, head_gain, filtered, stats, conv_gain, out_rec, out_conv):
    rows = 2 * BLK
    flat = lambda: pl.BlockSpec((rows, WIDE), lambda n: (group, 0))
    pair = pl.BlockSpec((BLK, WIDE), lambda n: (0, n))
    return pl.pallas_call(
        functools.partial(merge_kernel, group),
        grid=(4,),
        in_specs=[
            pl.BlockSpec(memory_space=pltpu.SMEM),
            flat(),
            flat(),
            flat(),
            pl.BlockSpec((2, 4, HEAD, HEAD), lambda n: (group, 0, 0, 0)),
            pl.BlockSpec((2, 8, WIDE), lambda n: (group, 0, 0)),
            pl.BlockSpec((4, HEAD, HEAD), lambda n: (0, 0, 0)),
            pl.BlockSpec((1, HEAD), lambda n: (0, 0)),
            flat(),
        ]
        + [pl.BlockSpec((8, 8 * BLK), lambda n: (0, 0))] * 4
        + [
            pl.BlockSpec((1, WIDE), lambda n: (0, 0)),
            pl.BlockSpec((WIDE, WIDE), lambda n: (0, n)),
            pl.BlockSpec((WIDE, WIDE), lambda n: (0, n)),
        ],
        out_specs=[pair, pair],
        out_shape=[jax.ShapeDtypeStruct((BLK, 2048), BF16)] * 2,
        scratch_shapes=[pltpu.VMEM((rows, 2 * WIDE), BF16)],
        compiler_params=params(),
        cost_estimate=pl.CostEstimate(
            flops=2 * rows * 1024 * 2048 * 3, bytes_accessed=7 * 2**20, transcendentals=0
        ),
    )(place, near, query_near, rgate, starts, offsets, arrived, head_gain, filtered, *stats, conv_gain, out_rec, out_conv)


def permuted(value, perm):
    return lax.ppermute(value, "tp", perm)


def on_device(
    tokens,
    norm_gain,
    w_query,
    w_forget,
    w_value,
    w_rgate,
    w_glu_value,
    w_glu_gate,
    forget_gap,
    decay_shift,
    head_gain,
    conv_taps,
    conv_gain,
    out_rec,
    out_conv,
):
    ahead = [(i, (i + 1) % 4) for i in range(4)]
    behind = [(i, (i - 1) % 4) for i in range(4)]
    t = lax.axis_index("tp")
    place = lax.dynamic_index_in_dim(
        jnp.asarray(np.concatenate([PLACE_TABLE, SLOT_TABLE], axis=1)), t, 0, keepdims=False
    )

    a, b = tokens[:BLK], tokens[BLK:]
    from_back_a = permuted(a, ahead)
    from_front_b = permuted(b, behind)
    from_back_b = permuted(b, ahead)
    from_front_a = permuted(a, behind)
    far_a = permuted(from_back_a, ahead)
    far_b = permuted(from_front_b, behind)

    gain, gap = norm_gain[None, :], forget_gap[None, :]
    common = (place, gain, gap, decay_shift)
    weights = (w_forget, w_value, w_query, w_rgate, w_glu_value, w_glu_gate)
    bufs = project_whole(0, (a, b), *common, weights, None)
    bufs = project_whole(2, (from_back_a, from_front_b), *common, weights, bufs)
    bufs = project_whole(4, (from_back_b, from_front_a), *common, weights, bufs)
    *bufs, added, close = bufs
    fv, pack, starts, offsets = last_states((far_a, far_b), *common, weights[:2], added, close)
    arrived = arriving_states(pack)
    near, query_near, rgate, mixed = last_rest((far_a, far_b), *common, fv, (w_query, w_rgate, w_glu_value, w_glu_gate), bufs)

    edge = lax.dynamic_slice(mixed, (place[15] * BLK + BLK - 32, 0), (32, WIDE))
    halo = lax.ppermute(edge, "sp", [(i, i + 1) for i in range(31)])
    filtered, stats = filter_rows(place, mixed, halo, conv_taps)
    stats_all = [stats] + [permuted(stats, [(i, (i + d) % 4) for i in range(4)]) for d in (1, 2, 3)]

    part = functools.partial(
        merge, place=place, near=near, query_near=query_near, rgate=rgate, starts=starts, offsets=offsets,
        arrived=arrived, head_gain=head_gain[None, :], filtered=filtered, stats=stats_all,
        conv_gain=conv_gain[None, :], out_rec=out_rec, out_conv=out_conv,
    )
    total = lambda *parts: functools.reduce(jnp.add, [p.astype(F32) for p in parts]).astype(BF16)
    far_top, far_bottom = part(3)
    via_back = permuted(far_top, ahead)
    via_front = permuted(far_bottom, behind)
    back_a, front_b = part(1)
    got_b = permuted(front_b, ahead)
    got_a = permuted(back_a, behind)
    back_b, front_a = part(2)
    sum_a = permuted(total(front_a, via_back), ahead)
    sum_b = permuted(total(back_b, via_front), behind)
    own_a, own_b = part(0)
    return jnp.concatenate([total(own_a, got_a, sum_a), total(own_b, got_b, sum_b)], axis=0)


def solution(mesh):
    placed = (
        P(("sp", "tp"), None),
        P(),
        P(None, "tp"),
        P(None, "tp"),
        P(None, "tp"),
        P(None, "tp"),
        P(None, "tp"),
        P(None, "tp"),
        P("tp"),
        P("sp", "tp"),
        P(),
        P(None, "tp"),
        P("tp"),
        P("tp", None),
        P("tp", None),
    )
    return jax.shard_map(on_device, mesh=mesh, in_specs=placed, out_specs=P(("sp", "tp"), None), check_vma=False)
```

```python
import functools

import jax
import jax.numpy as jnp
import numpy as np
from jax import lax
from jax.experimental import pallas as pl
from jax.experimental.pallas import tpu as pltpu
from jax.sharding import PartitionSpec as P


HEAD = 128
BLK = 128
NORM_EPS = 1e-05
HEAD_EPS = 1e-06
F32 = jnp.float32
BF16 = jnp.bfloat16


SLOT = np.array([[0, 1], [5, 3], [6, 7], [2, 4]])
SLOT_TABLE = np.array(
    [[SLOT[(p // 2 - t) % 4][p % 2] for p in range(8)] for t in range(4)], dtype=np.int32
)
PLACE_TABLE = np.argsort(SLOT_TABLE, axis=1).astype(np.int32)


def params(**kw):
    return pltpu.CompilerParams(vmem_limit_bytes=58 * 1024 * 1024, **kw)


def dot(a, b, dims=((1,), (0,))):
    return lax.dot_general(a, b, (dims, ((), ())), preferred_element_type=F32)


def silu(x):
    return x * jax.nn.sigmoid(x)


WIDE = 4 * HEAD


def gates(forget, gap, shift):
    key = gap * jax.nn.sigmoid(-forget.astype(F32))
    spread = jnp.concatenate(
        [jnp.broadcast_to(shift[:, h : h + 1], (BLK, HEAD)) for h in range(4)], axis=1
    )
    log_forget = jnp.log1p(-key) + spread
    high = log_forget.astype(BF16)
    low = (log_forget - high.astype(F32)).astype(BF16)
    rows = lax.broadcasted_iota(jnp.int32, (BLK, BLK), 0)
    cols = lax.broadcasted_iota(jnp.int32, (BLK, BLK), 1)
    lower = (rows >= cols).astype(F32).astype(BF16)
    return key, dot(lower, high) + dot(lower, low)


def pieces(log_row):
    high = log_row.astype(BF16).astype(F32)
    mid = (log_row - high).astype(BF16).astype(F32)
    low = log_row - high - mid
    row = lax.broadcasted_iota(jnp.int32, (16, HEAD), 0)
    tile = jnp.where(row == 0, high, jnp.where(row == 1, mid, jnp.where(row == 2, low, 0.0)))
    return tile.astype(BF16)


def block_outputs(key, run, value, query, near, query_near, at):
    middle = run[BLK // 2 - 1 : BLK // 2, :]
    query_mid = silu(query.astype(F32)) * jnp.exp(run - middle)
    key_mid = (key * jnp.exp(middle - run)).astype(BF16)
    query_near[at, :] = (query_mid * jnp.exp(middle)).astype(BF16)
    query_mid = query_mid.astype(BF16)
    rows = lax.broadcasted_iota(jnp.int32, (BLK, BLK), 0)
    cols = lax.broadcasted_iota(jnp.int32, (BLK, BLK), 1)
    for h in range(4):
        lanes = slice(h * HEAD, (h + 1) * HEAD)
        scores = dot(query_mid[:, lanes], key_mid[:, lanes], ((1,), (1,)))
        scores = jnp.where(rows >= cols, scores, 0.0).astype(BF16)
        near[at, lanes] = dot(scores, value[:, lanes])


def fetch(pairs, sems):
    copies = [pltpu.make_async_copy(source, target, sems.at[k]) for k, (source, target) in enumerate(pairs)]
    for copy in copies:
        copy.start()
    return copies


def norm_kernel(tokens, gain, top, bottom):
    g = gain[...]
    for k, out in enumerate((top, bottom)):
        for r in range(0, BLK, 32):
            rows = tokens[k * BLK + r : k * BLK + r + 32, :].astype(F32)
            centred = rows - jnp.mean(rows, axis=-1, keepdims=True)
            var = jnp.mean(centred * centred, axis=-1, keepdims=True)
            out[r : r + 32, :] = (centred * lax.rsqrt(var + NORM_EPS) * g).astype(BF16)


def norm_rows(tokens, gain):
    half = jax.ShapeDtypeStruct((BLK, tokens.shape[1]), BF16)
    return pl.pallas_call(
        norm_kernel, out_shape=[half, half], compiler_params=params(), name="norm_rows"
    )(tokens, gain)


def glu(value, gate):
    return (value.astype(F32) * jax.nn.sigmoid(gate.astype(F32))).astype(BF16)


def keys_kernel(reuse, last, place, *refs):
    x_top, x_bottom, gap, shift_top, shift_bottom = refs[:5]
    weights, refs = refs[5:9], refs[9:]
    if last:
        added, close_all, fv, mixed, pack, starts, offsets, xbuf, wbuf, parts, sems, more = refs[2:]
    else:
        fv, mixed, added, close, xbuf, wbuf, sems = refs[4 if reuse else 0 :]
    copies = fetch(
        [(x_top, xbuf.at[pl.ds(0, BLK)]), (x_bottom, xbuf.at[pl.ds(BLK, BLK)])]
        + [(w, wbuf.at[k]) for k, w in enumerate(weights)],
        sems,
    )
    if last:
        bring_parts = pltpu.make_async_copy(added.at[pl.ds(0, 6)], parts.at[pl.ds(0, 6)], more.at[0])
        bring_parts.start()
    copies[0].wait()
    copies[1].wait()

    def times(n):
        copies[2 + n].wait()
        return dot(xbuf[...], wbuf[n]).astype(BF16)

    fv[:, 0:WIDE] = times(0)
    fv[:, WIDE : 2 * WIDE] = times(1)
    ends = []
    for k, shift in enumerate((shift_top, shift_bottom)):
        at = slice(k * BLK, (k + 1) * BLK)
        key, run = gates(fv[at, 0:WIDE], gap[...], shift[...])
        value = fv[at, WIDE : 2 * WIDE]
        end = run[BLK - 1 : BLK, :]
        key_far = (key * jnp.exp(end - run)).astype(BF16)
        ends.append(end)
        if not last:
            close[k] = jnp.broadcast_to(end, (8, WIDE))
        for h in range(4):
            lanes = slice(h * HEAD, (h + 1) * HEAD)
            sum_h = dot(value[:, lanes], key_far[:, lanes], ((0,), (0,)))
            if last:
                parts[6 + k, h] = sum_h
            else:
                added[k, h] = sum_h
    mixed[...] = glu(times(2), times(3))
    if last:
        bring_parts.wait()
        scan_blocks(place, ends, close_all, parts, pack, starts, offsets)


def scan_blocks(place, ends, close_all, parts, pack, starts, offsets):
    state = [jnp.zeros((HEAD, HEAD), F32) for _ in range(4)]
    total = jnp.zeros((1, WIDE), F32)
    for i in range(8):
        slot = place[8 + i]
        offsets[slot] = jnp.broadcast_to(total, (8, WIDE))
        end = jnp.where(
            slot == 6, ends[0], jnp.where(slot == 7, ends[1], close_all[jnp.minimum(slot, 5)][0:1, :])
        )
        keep = jnp.exp(end)
        for h in range(4):
            lanes = slice(h * HEAD, (h + 1) * HEAD)
            starts[slot, h] = state[h].astype(BF16)
            state[h] = state[h] * keep[:, lanes] + parts[slot, h]
        total = total + end
    for h in range(4):
        tile = pieces(total[:, h * HEAD : (h + 1) * HEAD])
        rows = state[h].astype(BF16)
        for j in range(8):
            pack[8 * h + j, 0:16, :] = rows[16 * j : 16 * j + 16, :]
            pack[8 * h + j, 16:32, :] = tile


def any_spec():
    return pl.BlockSpec(memory_space=pl.ANY)


def keys(group, x, place, gap, shift, weights, bufs):
    depth = x[0].shape[1]
    rows = 2 * BLK
    last = group == 3
    block = lambda *shape: pl.BlockSpec(shape, lambda i, p: (group,) + (0,) * (len(shape) - 1))
    whole = lambda *shape: pl.BlockSpec(shape, lambda i, p: (0,) * len(shape))
    array = jax.ShapeDtypeStruct
    out_specs = [block(rows, 2 * WIDE), block(rows, WIDE)]
    out_shape = [array((8 * BLK, 2 * WIDE), BF16), array((8 * BLK, WIDE), BF16)]
    scratch = [pltpu.VMEM((rows, depth), BF16), pltpu.VMEM((4, depth, WIDE), BF16)]
    if last:
        buf_specs = [any_spec()] * 3 + [whole(8, 8, WIDE)]
        out_specs += [whole(32, 32, HEAD), whole(8, 4, HEAD, HEAD), whole(8, 8, WIDE)]
        out_shape += [array((32, 32, HEAD), BF16), array((8, 4, HEAD, HEAD), BF16), array((8, 8, WIDE), F32)]
        scratch += [
            pltpu.VMEM((8, 4, HEAD, HEAD), F32),
            pltpu.SemaphoreType.DMA((6,)),
            pltpu.SemaphoreType.DMA((1,)),
        ]
    else:
        buf_specs = [any_spec()] * len(bufs)
        out_specs += [block(2, 4, HEAD, HEAD), block(2, 8, WIDE)]
        out_shape += [array((8, 4, HEAD, HEAD), F32), array((8, 8, WIDE), F32)]
        scratch += [pltpu.SemaphoreType.DMA((6,))]
    aliased = min(len(bufs), 2 if last else 4)
    return pl.pallas_call(
        functools.partial(keys_kernel, bool(bufs), last),
        grid_spec=pltpu.PrefetchScalarGridSpec(
            num_scalar_prefetch=1,
            grid=(1,),
            in_specs=[any_spec()] * 2
            + [whole(1, WIDE)]
            + [pl.BlockSpec((BLK, 4), lambda i, p, k=k: (p[2 * group + k], 0)) for k in range(2)]
            + [any_spec()] * 4
            + buf_specs,
            out_specs=out_specs,
            scratch_shapes=scratch,
        ),
        out_shape=out_shape,
        input_output_aliases={10 + k: k for k in range(aliased)},
        compiler_params=params(),
        cost_estimate=pl.CostEstimate(
            flops=2 * rows * depth * WIDE * 6, bytes_accessed=12 * 2**20, transcendentals=0
        ),
    )(place, *x, gap, shift, shift, *weights, *bufs)


def prefix_kernel(packs, arriving):
    state = jnp.zeros((16, HEAD), F32)
    for i in range(32):
        arriving[i] = state.astype(BF16)
        tile = packs[i, 16:32, :].astype(F32)
        log = tile[0:1] + tile[1:2] + tile[2:3]
        state = jnp.exp(log) * state + packs[i, 0:16, :].astype(F32)


def arriving_states(pack):
    packs = lax.all_to_all(pack, "sp", split_axis=0, concat_axis=0, tiled=True)
    arriving = pl.pallas_call(
        prefix_kernel,
        out_shape=jax.ShapeDtypeStruct((32, 16, HEAD), BF16),
        compiler_params=params(),
        cost_estimate=pl.CostEstimate(flops=10**8, bytes_accessed=2**20, transcendentals=0),
        name="prefix",
    )(packs)
    arrived = lax.all_to_all(arriving, "sp", split_axis=0, concat_axis=0, tiled=True)
    return arrived.reshape(4, HEAD, HEAD)


def filter_kernel(table, mixed, halo, taps, filtered, stats, window):
    i = pl.program_id(0)
    reach = 32

    @pl.when(i == 0)
    def _():
        window[0:reach, :] = halo[...].astype(F32)

    @pl.when(i > 0)
    def _():
        window[0:reach, :] = window[BLK : BLK + reach, :]

    window[reach : reach + BLK, :] = mixed[...].astype(F32)
    row_sum = jnp.zeros((BLK, HEAD), F32)
    row_square = jnp.zeros((BLK, HEAD), F32)
    for c in range(4):
        lanes = slice(c * HEAD, (c + 1) * HEAD)
        acc = jnp.zeros((BLK, HEAD), F32)
        for r in range(8):
            used = [q for q in range(5) if 0 <= 8 * q + r - 2 < 31]
            shifted = window[8 * used[0] + r : 8 * used[-1] + r + BLK, lanes]
            part = None
            for q in used:
                j, lead = 8 * q + r - 2, 8 * (q - used[0])
                term = taps[j : j + 1, lanes] * shifted[lead : lead + BLK, :]
                part = term if part is None else part + term
            acc = acc + part
        filtered[:, lanes] = acc
        row_sum = row_sum + acc
        row_square = row_square + acc * acc
    lane = lax.broadcasted_iota(jnp.int32, (BLK, HEAD), 1)
    tile = jnp.where(
        lane == 0,
        jnp.sum(row_sum, axis=1, keepdims=True),
        jnp.where(lane == 1, jnp.sum(row_square, axis=1, keepdims=True), 0.0),
    )
    stats[...] = jnp.transpose(tile)[0:8, :]


def filter_rows(place, mixed, halo, taps):
    return pl.pallas_call(
        filter_kernel,
        grid_spec=pltpu.PrefetchScalarGridSpec(
            num_scalar_prefetch=1,
            grid=(8,),
            in_specs=[
                pl.BlockSpec((BLK, WIDE), lambda i, p: (p[8 + i], 0)),
                pl.BlockSpec((32, WIDE), lambda i, p: (0, 0)),
                pl.BlockSpec((31, WIDE), lambda i, p: (0, 0)),
            ],
            out_specs=[
                pl.BlockSpec((BLK, WIDE), lambda i, p: (p[8 + i], 0)),
                pl.BlockSpec((8, BLK), lambda i, p: (0, i)),
            ],
            scratch_shapes=[pltpu.VMEM((32 + BLK, WIDE), F32)],
        ),
        out_shape=[
            jax.ShapeDtypeStruct((8 * BLK, WIDE), F32),
            jax.ShapeDtypeStruct((8, 8 * BLK), F32),
        ],
        compiler_params=params(),
        cost_estimate=pl.CostEstimate(flops=7 * 10**9, bytes_accessed=5 * 2**20, transcendentals=0),
        name="filter_rows",
    )(place, mixed, halo, taps)


def merge_kernel(group, place, x_top, x_bottom, fv, gap, shift_top, shift_bottom, starts, offsets, arrived, head_gain, filtered, s0, s1, s2, s3, conv_gain, w_query, w_rgate, w_rec, w_conv, top, bottom, xbuf, wbuf, obuf, query, rgate, near, query_near, act, sems):
    copies = fetch(
        [
            (x_top, xbuf.at[pl.ds(0, BLK)]),
            (x_bottom, xbuf.at[pl.ds(BLK, BLK)]),
            (w_query, wbuf.at[0]),
            (w_rgate, wbuf.at[1]),
            (w_rec, obuf.at[0]),
            (w_conv, obuf.at[1]),
        ],
        sems,
    )
    for k in range(3):
        copies[k].wait()
    query[...] = dot(xbuf[...], wbuf[0]).astype(BF16)
    copies[3].wait()
    rgate[...] = dot(xbuf[...], wbuf[1]).astype(BF16)
    for k, shift in enumerate((shift_top, shift_bottom)):
        rows = slice(k * BLK, (k + 1) * BLK)
        key, run = gates(fv[rows, 0:WIDE], gap[...], shift[...])
        block_outputs(key, run, fv[rows, WIDE : 2 * WIDE], query[rows, :], near, query_near, rows)
        carry = jnp.exp(offsets[k, 0:1, :])
        for h in range(4):
            lanes = slice(h * HEAD, (h + 1) * HEAD)
            state = starts[k, h].astype(F32) + carry[:, lanes] * arrived[h].astype(F32)
            rec = near[rows, lanes] + dot(query_near[rows, lanes], state.astype(BF16), ((1,), (1,)))
            rec = rec * lax.rsqrt(jnp.mean(rec * rec, axis=-1, keepdims=True) + HEAD_EPS)
            rec = rec * head_gain[...] * silu(rgate[rows, lanes].astype(F32))
            act[rows, lanes] = rec.astype(BF16)
        at = pl.ds(pl.multiple_of(place[2 * group + k] * BLK, BLK), BLK)
        stats = (s0[:, at] + s1[:, at]) + (s2[:, at] + s3[:, at])
        tile = jnp.transpose(jnp.concatenate([stats] * 16, axis=0))
        mean = tile[:, 0:1] / 2048.0
        scale = lax.rsqrt(tile[:, 1:2] / 2048.0 - mean * mean + NORM_EPS)
        normed = (filtered[rows, :] - mean) * scale * conv_gain[...]
        act[rows, WIDE : 2 * WIDE] = silu(normed).astype(BF16)
    copies[4].wait()
    copies[5].wait()
    for n in range(4):
        cols = slice(n * 512, (n + 1) * 512)
        part = dot(act[:, 0:WIDE], obuf[0, :, cols]) + dot(act[:, WIDE : 2 * WIDE], obuf[1, :, cols])
        top[:, cols] = part[0:BLK, :].astype(BF16)
        bottom[:, cols] = part[BLK : 2 * BLK, :].astype(BF16)


def merge(group, x, place, fv, gap, shift, starts, offsets, arrived, head_gain, filtered, stats, conv_gain, w_query, w_rgate, out_rec, out_conv):
    rows = 2 * BLK
    depth, width = w_query.shape[0], out_rec.shape[1]
    block = lambda *shape: pl.BlockSpec(shape, lambda i, p: (group,) + (0,) * (len(shape) - 1))
    whole = lambda *shape: pl.BlockSpec(shape, lambda i, p: (0,) * len(shape))
    return pl.pallas_call(
        functools.partial(merge_kernel, group),
        grid_spec=pltpu.PrefetchScalarGridSpec(
            num_scalar_prefetch=1,
            grid=(1,),
            in_specs=[any_spec()] * 2
            + [block(rows, 2 * WIDE), whole(1, WIDE)]
            + [pl.BlockSpec((BLK, 4), lambda i, p, k=k: (p[2 * group + k], 0)) for k in range(2)]
            + [block(2, 4, HEAD, HEAD), block(2, 8, WIDE), whole(4, HEAD, HEAD), whole(1, HEAD)]
            + [block(rows, WIDE)]
            + [whole(8, 8 * BLK)] * 4
            + [whole(1, WIDE)]
            + [any_spec()] * 4,
            out_specs=[whole(BLK, width), whole(BLK, width)],
            scratch_shapes=[
                pltpu.VMEM((rows, depth), BF16),
                pltpu.VMEM((2, depth, WIDE), BF16),
                pltpu.VMEM((2, WIDE, width), BF16),
                pltpu.VMEM((rows, WIDE), BF16),
                pltpu.VMEM((rows, WIDE), BF16),
                pltpu.VMEM((rows, WIDE), F32),
                pltpu.VMEM((rows, WIDE), BF16),
                pltpu.VMEM((rows, 2 * WIDE), BF16),
                pltpu.SemaphoreType.DMA((6,)),
            ],
        ),
        out_shape=[jax.ShapeDtypeStruct((BLK, width), BF16)] * 2,
        compiler_params=params(),
        cost_estimate=pl.CostEstimate(
            flops=2 * rows * 1024 * 2048 * 6, bytes_accessed=10 * 2**20, transcendentals=0
        ),
    )(place, *x, fv, gap, shift, shift, starts, offsets, arrived, head_gain, filtered, *stats, conv_gain, w_query, w_rgate, out_rec, out_conv)


def finish_kernel(own_a, got_a, sum_a, own_b, got_b, sum_b, out):
    for k, parts in enumerate(((own_a, got_a, sum_a), (own_b, got_b, sum_b))):
        total = sum(p[...].astype(F32) for p in parts[1:]) + parts[0][...].astype(F32)
        out[k * BLK : (k + 1) * BLK, :] = total.astype(BF16)


def finish(*parts):
    width = parts[0].shape[1]
    return pl.pallas_call(
        finish_kernel,
        grid=(4,),
        in_specs=[pl.BlockSpec((BLK, width // 4), lambda n: (0, n))] * 6,
        out_specs=pl.BlockSpec((2 * BLK, width // 4), lambda n: (0, n)),
        out_shape=jax.ShapeDtypeStruct((2 * BLK, width), BF16),
        compiler_params=params(),
        name="finish",
    )(*parts)


def permuted(value, perm):
    return lax.ppermute(value, "tp", perm)


def on_device(
    tokens,
    norm_gain,
    w_query,
    w_forget,
    w_value,
    w_rgate,
    w_glu_value,
    w_glu_gate,
    forget_gap,
    decay_shift,
    head_gain,
    conv_taps,
    conv_gain,
    out_rec,
    out_conv,
):
    ahead = [(i, (i + 1) % 4) for i in range(4)]
    behind = [(i, (i - 1) % 4) for i in range(4)]
    t = lax.axis_index("tp")
    place = lax.dynamic_index_in_dim(
        jnp.asarray(np.concatenate([PLACE_TABLE, SLOT_TABLE], axis=1)), t, 0, keepdims=False
    )

    gap = forget_gap[None, :]
    a, b = norm_rows(tokens, norm_gain[None, :])
    from_back_a = permuted(a, ahead)
    from_front_b = permuted(b, behind)
    from_back_b = permuted(b, ahead)
    from_front_a = permuted(a, behind)
    far_a = permuted(from_back_a, ahead)
    far_b = permuted(from_front_b, behind)
    slots = ((a, b), (from_back_a, from_front_b), (from_back_b, from_front_a), (far_a, far_b))

    bufs = ()
    for group in range(3):
        bufs = keys(group, slots[group], place, gap, decay_shift, (w_forget, w_value, w_glu_value, w_glu_gate), bufs)
    fv, mixed, pack, starts, offsets = keys(
        3, slots[3], place, gap, decay_shift, (w_forget, w_value, w_glu_value, w_glu_gate), bufs
    )

    edge = lax.dynamic_slice(mixed, (place[15] * BLK + BLK - 32, 0), (32, WIDE))
    halo = lax.ppermute(edge, "sp", [(i, i + 1) for i in range(31)])
    arrived = arriving_states(pack)
    filtered, stats = filter_rows(place, mixed, halo, conv_taps)
    stats_all = [stats] + [permuted(stats, [(i, (i + d) % 4) for i in range(4)]) for d in (1, 2, 3)]

    part = functools.partial(
        merge, place=place, fv=fv, gap=gap, shift=decay_shift, starts=starts, offsets=offsets, arrived=arrived,
        head_gain=head_gain[None, :], filtered=filtered, stats=stats_all, conv_gain=conv_gain[None, :],
        w_query=w_query, w_rgate=w_rgate, out_rec=out_rec, out_conv=out_conv,
    )
    add = lambda x, y: (x.astype(F32) + y.astype(F32)).astype(BF16)
    far_top, far_bottom = part(3, slots[3])
    via_back = permuted(far_top, ahead)
    via_front = permuted(far_bottom, behind)
    back_a, front_b = part(1, slots[1])
    got_b = permuted(front_b, ahead)
    got_a = permuted(back_a, behind)
    back_b, front_a = part(2, slots[2])
    sum_a = permuted(add(front_a, via_back), ahead)
    sum_b = permuted(add(back_b, via_front), behind)
    own_a, own_b = part(0, slots[0])
    return finish(own_a, got_a, sum_a, own_b, got_b, sum_b)


def solution(mesh):
    placed = (
        P(("sp", "tp"), None),
        P(),
        P(None, "tp"),
        P(None, "tp"),
        P(None, "tp"),
        P(None, "tp"),
        P(None, "tp"),
        P(None, "tp"),
        P("tp"),
        P("sp", "tp"),
        P(),
        P(None, "tp"),
        P("tp"),
        P("tp", None),
        P("tp", None),
    )
    return jax.shard_map(on_device, mesh=mesh, in_specs=placed, out_specs=P(("sp", "tp"), None), check_vma=False)
```

```python
import functools

import jax
import jax.numpy as jnp
import numpy as np
from jax import lax
from jax.experimental import pallas as pl
from jax.experimental.pallas import tpu as pltpu
from jax.sharding import PartitionSpec as P


HEAD = 128
BLK = 128
NORM_EPS = 1e-05
HEAD_EPS = 1e-06
F32 = jnp.float32
BF16 = jnp.bfloat16


SLOT = np.array([[0, 1], [5, 3], [6, 7], [2, 4]])
SLOT_TABLE = np.array(
    [[SLOT[(p // 2 - t) % 4][p % 2] for p in range(8)] for t in range(4)], dtype=np.int32
)
PLACE_TABLE = np.argsort(SLOT_TABLE, axis=1).astype(np.int32)
PLACES = np.concatenate([PLACE_TABLE, SLOT_TABLE], axis=1).reshape(-1)


def block_of(t, places, slot):
    return places[16 * t[0] + slot]


def slot_of(t, places, block):
    return places[16 * t[0] + 8 + block]


def params(mib=8, **kw):
    return pltpu.CompilerParams(vmem_limit_bytes=mib * 1024 * 1024, **kw)


def dot(a, b, dims=((1,), (0,))):
    return lax.dot_general(a, b, (dims, ((), ())), preferred_element_type=F32)


def silu(x):
    return x * jax.nn.sigmoid(x)


WIDE = 4 * HEAD


def gates(forget, gap, shift):
    key = gap * jax.nn.sigmoid(-forget.astype(F32))
    columns = jnp.transpose(jnp.concatenate([shift] * (BLK // 4), axis=0))
    spread = jnp.concatenate(
        [jnp.broadcast_to(columns[:, h : h + 1], (BLK, HEAD)) for h in range(4)], axis=1
    )
    log_forget = jnp.log1p(-key) + spread
    high = log_forget.astype(BF16)
    low = (log_forget - high.astype(F32)).astype(BF16)
    rows = lax.broadcasted_iota(jnp.int32, (BLK, BLK), 0)
    cols = lax.broadcasted_iota(jnp.int32, (BLK, BLK), 1)
    lower = (rows >= cols).astype(F32).astype(BF16)
    return key, dot(lower, high) + dot(lower, low)


def pieces(log_row):
    high = log_row.astype(BF16).astype(F32)
    mid = (log_row - high).astype(BF16).astype(F32)
    low = log_row - high - mid
    row = lax.broadcasted_iota(jnp.int32, (16, HEAD), 0)
    tile = jnp.where(row == 0, high, jnp.where(row == 1, mid, jnp.where(row == 2, low, 0.0)))
    return tile.astype(BF16)


def block_outputs(key, run, value, query, near, query_near, at):
    middle = run[BLK // 2 - 1 : BLK // 2, :]
    query_mid = silu(query.astype(F32)) * jnp.exp(run - middle)
    key_mid = (key * jnp.exp(middle - run)).astype(BF16)
    query_near[at, :] = (query_mid * jnp.exp(middle)).astype(BF16)
    query_mid = query_mid.astype(BF16)
    rows = lax.broadcasted_iota(jnp.int32, (BLK, BLK), 0)
    cols = lax.broadcasted_iota(jnp.int32, (BLK, BLK), 1)
    for h in range(4):
        lanes = slice(h * HEAD, (h + 1) * HEAD)
        scores = dot(query_mid[:, lanes], key_mid[:, lanes], ((1,), (1,)))
        scores = jnp.where(rows >= cols, scores, 0.0).astype(BF16)
        near[at, lanes] = dot(scores, value[:, lanes])


def fetch(pairs, sems):
    copies = [pltpu.make_async_copy(source, target, sems.at[k]) for k, (source, target) in enumerate(pairs)]
    for copy in copies:
        copy.start()
    return copies


def norm_kernel(tokens, gain, top, bottom, rows_in, sems):
    halves = [pl.ds(0, BLK), pl.ds(BLK, BLK)]
    copies = fetch([(tokens.at[h], rows_in.at[h]) for h in halves], sems)
    g = gain[...]
    for k, out in enumerate((top, bottom)):
        copies[k].wait()
        for r in range(0, BLK, 16):
            rows = rows_in[k * BLK + r : k * BLK + r + 16, :].astype(F32)
            centred = rows - jnp.mean(rows, axis=-1, keepdims=True)
            var = jnp.mean(centred * centred, axis=-1, keepdims=True)
            out[r : r + 16, :] = (centred * lax.rsqrt(var + NORM_EPS) * g).astype(BF16)


def norm_rows(tokens, gain):
    half = jax.ShapeDtypeStruct((BLK, tokens.shape[1]), BF16)
    return pl.pallas_call(
        norm_kernel,
        in_specs=[hbm_spec(), pl.BlockSpec(gain.shape, lambda: (0, 0))],
        out_shape=[half, half],
        scratch_shapes=[pltpu.VMEM(tokens.shape, BF16), pltpu.SemaphoreType.DMA((2,))],
        compiler_params=params(58),
        name="norm_rows",
    )(tokens, gain)


def glu(value, gate):
    return (value.astype(F32) * jax.nn.sigmoid(gate.astype(F32))).astype(BF16)


def keys_kernel(first, last, t, places, *refs):
    x_top, x_bottom, gap, shift_top, shift_bottom = refs[:5]
    weights, refs = refs[5:9], refs[9:]
    if first:
        fv, mixed, added, close, xbuf, sems = refs
    elif last:
        mixed_in, added, close_all, fv, mixed, pack, starts, offsets, edge, xbuf, parts, tail, sems = refs[1:]
    else:
        fv, mixed, added, close, xbuf, sems = refs[4:]
    pairs = [(x_top, xbuf.at[pl.ds(0, BLK)]), (x_bottom, xbuf.at[pl.ds(BLK, BLK)])]
    if last:
        tail_slot = slot_of(t, places, 7)
        start = pl.multiple_of(jnp.minimum(tail_slot, 5) * BLK + BLK - 32, 32)
        pairs += [(added.at[pl.ds(0, 6)], parts.at[pl.ds(0, 6)]), (mixed_in.at[pl.ds(start, 32)], tail)]
    copies = fetch(pairs, sems)
    copies[0].wait()
    copies[1].wait()

    def times(n):
        return dot(xbuf[...], weights[n][...]).astype(BF16)

    fv[:, 0:WIDE] = times(0)
    fv[:, WIDE : 2 * WIDE] = times(1)
    ends = []
    for k, shift in enumerate((shift_top, shift_bottom)):
        at = slice(k * BLK, (k + 1) * BLK)
        key, run = gates(fv[at, 0:WIDE], gap[...], shift[...])
        value = fv[at, WIDE : 2 * WIDE]
        end = run[BLK - 1 : BLK, :]
        key_far = (key * jnp.exp(end - run)).astype(BF16)
        ends.append(end)
        if not last:
            close[k] = jnp.broadcast_to(end, (8, WIDE))
        for h in range(4):
            lanes = slice(h * HEAD, (h + 1) * HEAD)
            sum_h = dot(value[:, lanes], key_far[:, lanes], ((0,), (0,)))
            if last:
                parts[6 + k, h] = sum_h
            else:
                added[k, h] = sum_h
    mixed_now = glu(times(2), times(3))
    mixed[...] = mixed_now
    if last:
        copies[2].wait()
        copies[3].wait()
        edge[...] = jnp.where(
            tail_slot == 7, mixed_now[2 * BLK - 32 :, :].astype(F32), tail[...].astype(F32)
        ).astype(BF16)
        scan_blocks(t, places, ends, close_all, parts, pack, starts, offsets)


def scan_blocks(t, places, ends, close_all, parts, pack, starts, offsets):
    state = [jnp.zeros((HEAD, HEAD), F32) for _ in range(4)]
    total = jnp.zeros((1, WIDE), F32)
    for i in range(8):
        slot = slot_of(t, places, i)
        offsets[slot] = jnp.broadcast_to(total, (8, WIDE))
        end = jnp.where(
            slot == 6, ends[0], jnp.where(slot == 7, ends[1], close_all[jnp.minimum(slot, 5)][0:1, :])
        )
        keep = jnp.exp(end)
        for h in range(4):
            lanes = slice(h * HEAD, (h + 1) * HEAD)
            starts[slot, h] = state[h].astype(BF16)
            state[h] = state[h] * keep[:, lanes] + parts[slot, h]
        total = total + end
    for h in range(4):
        tile = pieces(total[:, h * HEAD : (h + 1) * HEAD])
        rows = state[h].astype(BF16)
        for j in range(8):
            pack[8 * h + j, 0:16, :] = rows[16 * j : 16 * j + 16, :]
            pack[8 * h + j, 16:24, :] = tile[0:8, :]


def any_spec():
    return pl.BlockSpec(memory_space=pl.ANY)


def hbm_spec():
    return pl.BlockSpec(memory_space=pltpu.HBM)


def keys(group, x, t, gap, shift, weights, bufs):
    depth = x[0].shape[1]
    rows = 2 * BLK
    first, last = group == 0, group == 3
    block = lambda *shape: pl.BlockSpec(shape, lambda i, t, p: (group,) + (0,) * (len(shape) - 1))
    whole = lambda *shape: pl.BlockSpec(shape, lambda i, t, p: (0,) * len(shape))
    array = jax.ShapeDtypeStruct
    out_specs = [block(rows, 2 * WIDE), block(rows, WIDE)]
    out_shape = [array((8 * BLK, 2 * WIDE), BF16), array((8 * BLK, WIDE), BF16)]
    scratch = [pltpu.VMEM((rows, depth), BF16)]
    weight_specs = [pl.BlockSpec(memory_space=pltpu.VMEM)] * 4
    if last:
        buf_specs = [any_spec(), any_spec(), any_spec(), whole(8, 8, WIDE)]
        out_specs += [whole(32, 24, HEAD), whole(8, 4, HEAD, HEAD), whole(8, 8, WIDE), whole(32, WIDE)]
        out_shape += [
            array((32, 24, HEAD), BF16),
            array((8, 4, HEAD, HEAD), BF16),
            array((8, 8, WIDE), F32),
            array((32, WIDE), BF16),
        ]
        scratch += [pltpu.VMEM((8, 4, HEAD, HEAD), F32), pltpu.VMEM((32, WIDE), BF16)]
    else:
        buf_specs = [any_spec()] * len(bufs)
        out_specs += [block(2, 4, HEAD, HEAD), block(2, 8, WIDE)]
        out_shape += [array((8, 4, HEAD, HEAD), F32), array((8, 8, WIDE), F32)]
    copies = 4 if last else 2
    aliased = min(len(bufs), 2 if last else 4)
    return pl.pallas_call(
        functools.partial(keys_kernel, first, last),
        grid_spec=pltpu.PrefetchScalarGridSpec(
            num_scalar_prefetch=2,
            grid=(1,),
            in_specs=[any_spec()] * 2
            + [whole(1, WIDE)]
            + [pl.BlockSpec((4, BLK), lambda i, t, p, k=k: (0, block_of(t, p, 2 * group + k))) for k in range(2)]
            + weight_specs
            + buf_specs,
            out_specs=out_specs,
            scratch_shapes=scratch + [pltpu.SemaphoreType.DMA((copies,))],
        ),
        out_shape=out_shape,
        input_output_aliases={11 + k: k for k in range(aliased)},
        compiler_params=params(28),
        cost_estimate=pl.CostEstimate(
            flops=2 * rows * depth * WIDE * 6, bytes_accessed=12 * 2**20, transcendentals=0
        ),
    )(t, jnp.asarray(PLACES), *x, gap, shift, shift, *weights, *bufs)


def prefix_kernel(packs, arriving):
    state = jnp.zeros((16, HEAD), F32)
    for i in range(32):
        arriving[i] = state.astype(BF16)
        tile = packs[i, 16:24, :].astype(F32)
        log = tile[0:1] + tile[1:2] + tile[2:3]
        state = jnp.exp(log) * state + packs[i, 0:16, :].astype(F32)


def arriving_states(pack):
    packs = lax.all_to_all(pack, "sp", split_axis=0, concat_axis=0, tiled=True)
    arriving = pl.pallas_call(
        prefix_kernel,
        out_shape=jax.ShapeDtypeStruct((32, 16, HEAD), BF16),
        compiler_params=params(),
        cost_estimate=pl.CostEstimate(flops=10**8, bytes_accessed=2**20, transcendentals=0),
        name="prefix",
    )(packs)
    arrived = lax.all_to_all(arriving, "sp", split_axis=0, concat_axis=0, tiled=True)
    return arrived.reshape(4, HEAD, HEAD)


def filter_kernel(t, places, mixed, halo, taps, filtered, stats, window, sums):
    i = pl.program_id(0)
    reach = 32

    @pl.when(i == 0)
    def _():
        window[0:reach, :] = halo[...].astype(F32)

    @pl.when(i > 0)
    def _():
        window[0:reach, :] = window[BLK : BLK + reach, :]

    window[reach : reach + BLK, :] = mixed[...].astype(F32)
    sums[...] = jnp.zeros_like(sums)

    def one(c, carry):
        lanes = pl.ds(pl.multiple_of(c * HEAD, HEAD), HEAD)
        acc = jnp.zeros((BLK, HEAD), F32)
        for r in range(8):
            used = [q for q in range(5) if 0 <= 8 * q + r - 2 < 31]
            shifted = window[8 * used[0] + r : 8 * used[-1] + r + BLK, lanes]
            part = None
            for q in used:
                j, lead = 8 * q + r - 2, 8 * (q - used[0])
                term = taps[j : j + 1, lanes] * shifted[lead : lead + BLK, :]
                part = term if part is None else part + term
            acc = acc + part
        filtered[:, lanes] = acc
        sums[0] = sums[0] + acc
        sums[1] = sums[1] + acc * acc
        return carry

    lax.fori_loop(0, 4, one, 0)
    lane = lax.broadcasted_iota(jnp.int32, (BLK, HEAD), 1)
    tile = jnp.where(
        lane == 0,
        jnp.sum(sums[0], axis=1, keepdims=True),
        jnp.where(lane == 1, jnp.sum(sums[1], axis=1, keepdims=True), 0.0),
    )
    stats[...] = jnp.transpose(tile)[0:8, :]


def filter_rows(t, mixed, halo, taps):
    return pl.pallas_call(
        filter_kernel,
        grid_spec=pltpu.PrefetchScalarGridSpec(
            num_scalar_prefetch=2,
            grid=(8,),
            in_specs=[
                pl.BlockSpec((BLK, WIDE), lambda i, t, p: (slot_of(t, p, i), 0)),
                pl.BlockSpec((32, WIDE), lambda i, t, p: (0, 0)),
                pl.BlockSpec((31, WIDE), lambda i, t, p: (0, 0)),
            ],
            out_specs=[
                pl.BlockSpec((BLK, WIDE), lambda i, t, p: (slot_of(t, p, i), 0)),
                pl.BlockSpec((8, BLK), lambda i, t, p: (0, i)),
            ],
            scratch_shapes=[pltpu.VMEM((32 + BLK, WIDE), F32), pltpu.VMEM((2, BLK, HEAD), F32)],
        ),
        out_shape=[
            jax.ShapeDtypeStruct((8 * BLK, WIDE), F32),
            jax.ShapeDtypeStruct((8, 8 * BLK), F32),
        ],
        compiler_params=params(58),
        cost_estimate=pl.CostEstimate(flops=7 * 10**9, bytes_accessed=5 * 2**20, transcendentals=0),
        name="filter_rows",
    )(t, jnp.asarray(PLACES), mixed, halo, taps)


QUERY_SCRATCH = [((2 * BLK, 2048), BF16), ((2, 2048, WIDE), BF16), ((2 * BLK, 2 * WIDE), BF16), ((2 * BLK, WIDE), BF16)]
NEAR_SCRATCH = [((2 * BLK, WIDE), F32), ((2 * BLK, WIDE), BF16), ((2 * BLK, WIDE), BF16)]


def rows_of(ref, group, size):
    return ref.at[pl.ds(group * size, size)]


def query_side(group, later, ins, scratch, outs, sems):
    x_top, x_bottom, fv_all, w_query, w_rgate, gap, *shifts = ins
    xbuf, wbuf, fv, query = scratch
    near, query_near, rgate = outs
    copies = fetch(
        [
            (x_top, xbuf.at[pl.ds(0, BLK)]),
            (x_bottom, xbuf.at[pl.ds(BLK, BLK)]),
            (w_query, wbuf.at[0]),
            (rows_of(fv_all, group, 2 * BLK), fv),
            (w_rgate, wbuf.at[1]),
        ],
        sems,
    )
    for k in range(3):
        copies[k].wait()
    more = later()
    query[...] = dot(xbuf[...], wbuf[0]).astype(BF16)
    copies[3].wait()
    for k, shift in enumerate(shifts):
        rows = slice(k * BLK, (k + 1) * BLK)
        key, run = gates(fv[rows, 0:WIDE], gap[...], shift[...])
        block_outputs(key, run, fv[rows, WIDE : 2 * WIDE], query[rows, :], near, query_near, rows)
    copies[4].wait()
    rgate[...] = dot(xbuf[...], wbuf[1]).astype(BF16)
    return more


def query_kernel(group, t, places, *refs):
    outs, scratch, sems = refs[8:11], refs[11:15], refs[15]
    query_side(group, lambda: None, refs[:8], scratch, outs, sems)


def query_specs(group):
    return (
        [hbm_spec()] * 5
        + [pl.BlockSpec((1, WIDE), lambda i, t, p: (0, 0))]
        + [pl.BlockSpec((4, BLK), lambda i, t, p, k=k: (0, block_of(t, p, 2 * group + k))) for k in range(2)]
    )


def query_rows(group, x, t, fv, gap, shift, w_query, w_rgate):
    return pl.pallas_call(
        functools.partial(query_kernel, group),
        grid_spec=pltpu.PrefetchScalarGridSpec(
            num_scalar_prefetch=2,
            grid=(1,),
            in_specs=query_specs(group),
            out_specs=[pl.BlockSpec((2 * BLK, WIDE), lambda i, t, p: (0, 0))] * 3,
            scratch_shapes=[pltpu.VMEM(*v) for v in QUERY_SCRATCH] + [pltpu.SemaphoreType.DMA((5,))],
        ),
        out_shape=[jax.ShapeDtypeStruct((2 * BLK, WIDE), kind) for kind in (F32, BF16, BF16)],
        compiler_params=params(58),
        cost_estimate=pl.CostEstimate(
            flops=2 * 2 * BLK * 2048 * WIDE * 4, bytes_accessed=6 * 2**20, transcendentals=0
        ),
    )(t, jnp.asarray(PLACES), *x, fv, w_query, w_rgate, gap, shift, shift)


MERGE_SCRATCH = [
    ((2, WIDE, 2048), BF16),
    ((2, 4, HEAD, HEAD), BF16),
    ((2, 8, WIDE), F32),
    ((4, HEAD, HEAD), BF16),
    ((2 * BLK, WIDE), F32),
    ((4, 8, 8 * BLK), F32),
    ((2 * BLK, 2 * WIDE), BF16),
]


def merge_kernel(group, split, t, places, *refs):
    lead, refs = (refs[:3], refs[3:]) if split else (refs[:8], refs[8:])
    starts_all, offsets_all, arrived_all, filtered_all, *stats_all = refs[:8]
    w_rec, w_conv, head_gain, conv_gain, top, bottom = refs[8:14]
    obuf, starts, offsets, arrived, filtered, stats_buf, act = refs[14:21]
    near, query_near, rgate = refs[21:24]
    sems, refs = refs[24], refs[25:]

    def later():
        return fetch(
            [
                (rows_of(starts_all, group, 2), starts),
                (rows_of(offsets_all, group, 2), offsets),
                (arrived_all, arrived),
                (rows_of(filtered_all, group, 2 * BLK), filtered),
            ]
            + [(s, stats_buf.at[k]) for k, s in enumerate(stats_all)]
            + [(w_rec, obuf.at[0]), (w_conv, obuf.at[1])],
            sems,
        )

    if split:
        first = fetch(list(zip(lead, (near, query_near, rgate))), refs[0])
        more = later()
        for copy in first:
            copy.wait()
    else:
        more = query_side(group, later, lead, refs[:4], (near, query_near, rgate), refs[4])
    for copy in more[:8]:
        copy.wait()
    for k in range(2):
        rows = slice(k * BLK, (k + 1) * BLK)
        carry = jnp.exp(offsets[k, 0:1, :])
        for h in range(4):
            lanes = slice(h * HEAD, (h + 1) * HEAD)
            state = starts[k, h].astype(F32) + carry[:, lanes] * arrived[h].astype(F32)
            rec = near[rows, lanes] + dot(query_near[rows, lanes], state.astype(BF16), ((1,), (1,)))
            rec = rec * lax.rsqrt(jnp.mean(rec * rec, axis=-1, keepdims=True) + HEAD_EPS)
            rec = rec * head_gain[...] * silu(rgate[rows, lanes].astype(F32))
            act[rows, lanes] = rec.astype(BF16)
        at = pl.ds(pl.multiple_of(block_of(t, places, 2 * group + k) * BLK, BLK), BLK)
        stats = (stats_buf[0, :, at] + stats_buf[1, :, at]) + (stats_buf[2, :, at] + stats_buf[3, :, at])
        tile = jnp.transpose(jnp.concatenate([stats] * 16, axis=0))
        mean = tile[:, 0:1] / 2048.0
        scale = lax.rsqrt(tile[:, 1:2] / 2048.0 - mean * mean + NORM_EPS)
        normed = (filtered[rows, :] - mean) * scale * conv_gain[...]
        act[rows, WIDE : 2 * WIDE] = silu(normed).astype(BF16)
    more[8].wait()
    more[9].wait()
    for n in range(4):
        cols = slice(n * 512, (n + 1) * 512)
        part = dot(act[:, 0:WIDE], obuf[0, :, cols]) + dot(act[:, WIDE : 2 * WIDE], obuf[1, :, cols])
        top[:, cols] = part[0:BLK, :].astype(BF16)
        bottom[:, cols] = part[BLK : 2 * BLK, :].astype(BF16)


def merge(group, x, t, fv, gap, shift, starts, offsets, arrived, head_gain, filtered, stats, conv_gain, w_query, w_rgate, out_rec, out_conv, ready=None):
    width = out_rec.shape[1]
    split = ready is not None
    whole = lambda *shape: pl.BlockSpec(shape, lambda i, t, p: (0,) * len(shape))
    scratch = [pltpu.VMEM(*v) for v in MERGE_SCRATCH + NEAR_SCRATCH] + [pltpu.SemaphoreType.DMA((10,))]
    if split:
        lead, lead_specs = ready, [hbm_spec()] * 3
        scratch += [pltpu.SemaphoreType.DMA((3,))]
    else:
        lead, lead_specs = (*x, fv, w_query, w_rgate, gap, shift, shift), query_specs(group)
        scratch += [pltpu.VMEM(*v) for v in QUERY_SCRATCH] + [pltpu.SemaphoreType.DMA((5,))]
    return pl.pallas_call(
        functools.partial(merge_kernel, group, split),
        grid_spec=pltpu.PrefetchScalarGridSpec(
            num_scalar_prefetch=2,
            grid=(1,),
            in_specs=lead_specs + [hbm_spec()] * 10 + [whole(1, HEAD), whole(1, WIDE)],
            out_specs=[whole(BLK, width), whole(BLK, width)],
            scratch_shapes=scratch,
        ),
        out_shape=[jax.ShapeDtypeStruct((BLK, width), BF16)] * 2,
        compiler_params=params(58),
        cost_estimate=pl.CostEstimate(
            flops=2 * 2 * BLK * 1024 * 2048 * 6, bytes_accessed=10 * 2**20, transcendentals=0
        ),
    )(t, jnp.asarray(PLACES), *lead, starts, offsets, arrived, filtered, *stats, out_rec, out_conv, head_gain, conv_gain)


def finish_kernel(own_a, got_a, sum_a, own_b, got_b, sum_b, out):
    for k, parts in enumerate(((own_a, got_a, sum_a), (own_b, got_b, sum_b))):
        total = sum(p[...].astype(F32) for p in parts[1:]) + parts[0][...].astype(F32)
        out[k * BLK : (k + 1) * BLK, :] = total.astype(BF16)


def finish(*parts):
    width = parts[0].shape[1]
    return pl.pallas_call(
        finish_kernel,
        grid=(4,),
        in_specs=[pl.BlockSpec((BLK, width // 4), lambda n: (0, n))] * 6,
        out_specs=pl.BlockSpec((2 * BLK, width // 4), lambda n: (0, n)),
        out_shape=jax.ShapeDtypeStruct((2 * BLK, width), BF16),
        compiler_params=params(),
        name="finish",
    )(*parts)


def permuted(value, perm):
    return lax.ppermute(value, "tp", perm)


def on_device(
    tokens,
    norm_gain,
    w_query,
    w_forget,
    w_value,
    w_rgate,
    w_glu_value,
    w_glu_gate,
    forget_gap,
    decay_shift,
    head_gain,
    conv_taps,
    conv_gain,
    out_rec,
    out_conv,
):
    ahead = [(i, (i + 1) % 4) for i in range(4)]
    behind = [(i, (i - 1) % 4) for i in range(4)]
    t = lax.axis_index("tp").astype(jnp.int32).reshape(1)
    gap, shift = forget_gap[None, :], decay_shift.T
    a, b = norm_rows(tokens, norm_gain[None, :])
    from_back_a = permuted(a, ahead)
    from_front_b = permuted(b, behind)
    from_back_b = permuted(b, ahead)
    from_front_a = permuted(a, behind)
    far_a = permuted(from_back_a, ahead)
    far_b = permuted(from_front_b, behind)
    slots = ((a, b), (from_back_a, from_front_b), (from_back_b, from_front_a), (far_a, far_b))

    weights = (w_forget, w_value, w_glu_value, w_glu_gate)
    bufs = ()
    for group in range(3):
        bufs = keys(group, slots[group], t, gap, shift, weights, bufs)
    fv, mixed, pack, starts, offsets, edge = keys(3, slots[3], t, gap, shift, weights, bufs)

    halo = lax.ppermute(edge, "sp", [(i, i + 1) for i in range(31)])
    arrived = arriving_states(pack)
    filtered, stats = filter_rows(t, mixed, halo, conv_taps)
    stats_all = [stats] + [permuted(stats, [(i, (i + d) % 4) for i in range(4)]) for d in (1, 2, 3)]
    ready = query_rows(3, slots[3], t, fv, gap, shift, w_query, w_rgate)

    part = functools.partial(
        merge, t=t, fv=fv, gap=gap, shift=shift, starts=starts, offsets=offsets, arrived=arrived,
        head_gain=head_gain[None, :], filtered=filtered, stats=stats_all, conv_gain=conv_gain[None, :],
        w_query=w_query, w_rgate=w_rgate, out_rec=out_rec, out_conv=out_conv,
    )
    add = lambda x, y: (x.astype(F32) + y.astype(F32)).astype(BF16)
    far_top, far_bottom = part(3, slots[3], ready=ready)
    via_back = permuted(far_top, ahead)
    via_front = permuted(far_bottom, behind)
    back_a, front_b = part(1, slots[1])
    got_b = permuted(front_b, ahead)
    got_a = permuted(back_a, behind)
    back_b, front_a = part(2, slots[2])
    sum_a = permuted(add(front_a, via_back), ahead)
    sum_b = permuted(add(back_b, via_front), behind)
    own_a, own_b = part(0, slots[0])
    return finish(own_a, got_a, sum_a, own_b, got_b, sum_b)


def solution(mesh):
    placed = (
        P(("sp", "tp"), None),
        P(),
        P(None, "tp"),
        P(None, "tp"),
        P(None, "tp"),
        P(None, "tp"),
        P(None, "tp"),
        P(None, "tp"),
        P("tp"),
        P("sp", "tp"),
        P(),
        P(None, "tp"),
        P("tp"),
        P("tp", None),
        P("tp", None),
    )
    return jax.shard_map(on_device, mesh=mesh, in_specs=placed, out_specs=P(("sp", "tp"), None), check_vma=False)
```

```python
import functools

import jax
import jax.numpy as jnp
import numpy as np
from jax import lax
from jax.experimental import pallas as pl
from jax.experimental.pallas import tpu as pltpu
from jax.sharding import PartitionSpec as P


HEAD = 128
BLK = 128
NORM_EPS = 1e-05
HEAD_EPS = 1e-06
F32 = jnp.float32
BF16 = jnp.bfloat16


SLOT = np.array([[0, 1], [5, 3], [6, 7], [2, 4]])
SLOT_TABLE = np.array(
    [[SLOT[(p // 2 - t) % 4][p % 2] for p in range(8)] for t in range(4)], dtype=np.int32
)
PLACE_TABLE = np.argsort(SLOT_TABLE, axis=1).astype(np.int32)
PLACES = np.concatenate([PLACE_TABLE, SLOT_TABLE], axis=1).reshape(-1)


def block_of(t, places, slot):
    return places[16 * t[0] + slot]


def slot_of(t, places, block):
    return places[16 * t[0] + 8 + block]


LIMITS = {"norm": 8, "keys": 28, "last": 28, "filter": 58, "prefix": 50, "query": 58, "merge_3": 16, "merge": 24, "merge_0": 24}


def params(kind):
    return pltpu.CompilerParams(vmem_limit_bytes=LIMITS[kind] * 1024 * 1024)


def dot(a, b, dims=((1,), (0,))):
    return lax.dot_general(a, b, (dims, ((), ())), preferred_element_type=F32)


def silu(x):
    return x * jax.nn.sigmoid(x)


WIDE = 4 * HEAD


def gates(forget, gap, shift):
    key = gap * jax.nn.sigmoid(-forget.astype(F32))
    columns = jnp.transpose(jnp.concatenate([shift] * (BLK // 4), axis=0))
    spread = jnp.concatenate(
        [jnp.broadcast_to(columns[:, h : h + 1], (BLK, HEAD)) for h in range(4)], axis=1
    )
    log_forget = jnp.log1p(-key) + spread
    high = log_forget.astype(BF16)
    low = (log_forget - high.astype(F32)).astype(BF16)
    rows = lax.broadcasted_iota(jnp.int32, (BLK, BLK), 0)
    cols = lax.broadcasted_iota(jnp.int32, (BLK, BLK), 1)
    lower = (rows >= cols).astype(F32).astype(BF16)
    return key, dot(lower, high) + dot(lower, low)


def pieces(log_row):
    high = log_row.astype(BF16).astype(F32)
    mid = (log_row - high).astype(BF16).astype(F32)
    low = log_row - high - mid
    row = lax.broadcasted_iota(jnp.int32, (16, HEAD), 0)
    tile = jnp.where(row == 0, high, jnp.where(row == 1, mid, jnp.where(row == 2, low, 0.0)))
    return tile.astype(BF16)


def block_outputs(key, run, value, query, near, query_near, at):
    middle = run[BLK // 2 - 1 : BLK // 2, :]
    query_mid = silu(query.astype(F32)) * jnp.exp(run - middle)
    key_mid = (key * jnp.exp(middle - run)).astype(BF16)
    query_near[at, :] = (query_mid * jnp.exp(middle)).astype(BF16)
    query_mid = query_mid.astype(BF16)
    rows = lax.broadcasted_iota(jnp.int32, (BLK, BLK), 0)
    cols = lax.broadcasted_iota(jnp.int32, (BLK, BLK), 1)
    for h in range(4):
        lanes = slice(h * HEAD, (h + 1) * HEAD)
        scores = dot(query_mid[:, lanes], key_mid[:, lanes], ((1,), (1,)))
        scores = jnp.where(rows >= cols, scores, 0.0).astype(BF16)
        near[at, lanes] = dot(scores, value[:, lanes])


def fetch(pairs, sems):
    copies = [pltpu.make_async_copy(source, target, sems.at[k]) for k, (source, target) in enumerate(pairs)]
    for copy in copies:
        copy.start()
    return copies


def norm_kernel(tokens, gain, top, bottom, rows_in, sems):
    halves = [pl.ds(0, BLK), pl.ds(BLK, BLK)]
    copies = fetch([(tokens.at[h], rows_in.at[h]) for h in halves], sems)
    g = gain[...]
    for k, out in enumerate((top, bottom)):
        copies[k].wait()
        for r in range(0, BLK, 16):
            rows = rows_in[k * BLK + r : k * BLK + r + 16, :].astype(F32)
            centred = rows - jnp.mean(rows, axis=-1, keepdims=True)
            var = jnp.mean(centred * centred, axis=-1, keepdims=True)
            out[r : r + 16, :] = (centred * lax.rsqrt(var + NORM_EPS) * g).astype(BF16)


def norm_rows(tokens, gain):
    half = jax.ShapeDtypeStruct((BLK, tokens.shape[1]), BF16)
    return pl.pallas_call(
        norm_kernel,
        in_specs=[hbm_spec(), pl.BlockSpec(gain.shape, lambda: (0, 0))],
        out_shape=[half, half],
        scratch_shapes=[pltpu.VMEM(tokens.shape, BF16), pltpu.SemaphoreType.DMA((2,))],
        compiler_params=params("norm"),
        name="norm_rows",
    )(tokens, gain)


def glu(value, gate):
    return (value.astype(F32) * jax.nn.sigmoid(gate.astype(F32))).astype(BF16)


def keys_kernel(first, last, t, places, *refs):
    x_top, x_bottom, gap, shift_top, shift_bottom = refs[:5]
    weights, refs = refs[5:9], refs[9:]
    if first:
        fv, mixed, added, close, xbuf, sems = refs
    elif last:
        mixed_in, added, close_all, fv, mixed, pack, starts, offsets, edge, xbuf, parts, tail, sems = refs[1:]
    else:
        fv, mixed, added, close, xbuf, sems = refs[4:]
    pairs = [(x_top, xbuf.at[pl.ds(0, BLK)]), (x_bottom, xbuf.at[pl.ds(BLK, BLK)])]
    if last:
        tail_slot = slot_of(t, places, 7)
        start = pl.multiple_of(jnp.minimum(tail_slot, 5) * BLK + BLK - 32, 32)
        pairs += [(added.at[pl.ds(0, 6)], parts.at[pl.ds(0, 6)]), (mixed_in.at[pl.ds(start, 32)], tail)]
    copies = fetch(pairs, sems)
    copies[0].wait()
    copies[1].wait()

    def times(n):
        return dot(xbuf[...], weights[n][...]).astype(BF16)

    fv[:, 0:WIDE] = times(0)
    fv[:, WIDE : 2 * WIDE] = times(1)
    ends = []
    for k, shift in enumerate((shift_top, shift_bottom)):
        at = slice(k * BLK, (k + 1) * BLK)
        key, run = gates(fv[at, 0:WIDE], gap[...], shift[...])
        value = fv[at, WIDE : 2 * WIDE]
        end = run[BLK - 1 : BLK, :]
        key_far = (key * jnp.exp(end - run)).astype(BF16)
        ends.append(end)
        if not last:
            close[k] = jnp.broadcast_to(end, (8, WIDE))
        for h in range(4):
            lanes = slice(h * HEAD, (h + 1) * HEAD)
            sum_h = dot(value[:, lanes], key_far[:, lanes], ((0,), (0,)))
            if last:
                parts[6 + k, h] = sum_h
            else:
                added[k, h] = sum_h
    mixed_now = glu(times(2), times(3))
    mixed[...] = mixed_now
    if last:
        copies[2].wait()
        copies[3].wait()
        edge[...] = jnp.where(
            tail_slot == 7, mixed_now[2 * BLK - 32 :, :].astype(F32), tail[...].astype(F32)
        ).astype(BF16)
        scan_blocks(t, places, ends, close_all, parts, pack, starts, offsets)


def scan_blocks(t, places, ends, close_all, parts, pack, starts, offsets):
    state = [jnp.zeros((HEAD, HEAD), F32) for _ in range(4)]
    total = jnp.zeros((1, WIDE), F32)
    for i in range(8):
        slot = slot_of(t, places, i)
        offsets[slot] = jnp.broadcast_to(total, (8, WIDE))
        end = jnp.where(
            slot == 6, ends[0], jnp.where(slot == 7, ends[1], close_all[jnp.minimum(slot, 5)][0:1, :])
        )
        keep = jnp.exp(end)
        for h in range(4):
            lanes = slice(h * HEAD, (h + 1) * HEAD)
            starts[slot, h] = state[h].astype(BF16)
            state[h] = state[h] * keep[:, lanes] + parts[slot, h]
        total = total + end
    for h in range(4):
        tile = pieces(total[:, h * HEAD : (h + 1) * HEAD])
        rows = state[h].astype(BF16)
        for j in range(8):
            pack[8 * h + j, 0:16, :] = rows[16 * j : 16 * j + 16, :]
            pack[8 * h + j, 16:24, :] = tile[0:8, :]


def any_spec():
    return pl.BlockSpec(memory_space=pl.ANY)


def hbm_spec():
    return pl.BlockSpec(memory_space=pltpu.HBM)


def keys(group, x, t, gap, shift, weights, bufs):
    depth = x[0].shape[1]
    rows = 2 * BLK
    first, last = group == 0, group == 3
    block = lambda *shape: pl.BlockSpec(shape, lambda i, t, p: (group,) + (0,) * (len(shape) - 1))
    whole = lambda *shape: pl.BlockSpec(shape, lambda i, t, p: (0,) * len(shape))
    array = jax.ShapeDtypeStruct
    out_specs = [block(rows, 2 * WIDE), block(rows, WIDE)]
    out_shape = [array((8 * BLK, 2 * WIDE), BF16), array((8 * BLK, WIDE), BF16)]
    scratch = [pltpu.VMEM((rows, depth), BF16)]
    weight_specs = [pl.BlockSpec(memory_space=pltpu.VMEM)] * 4
    if last:
        buf_specs = [any_spec(), any_spec(), any_spec(), whole(8, 8, WIDE)]
        out_specs += [whole(32, 24, HEAD), whole(8, 4, HEAD, HEAD), whole(8, 8, WIDE), whole(32, WIDE)]
        out_shape += [
            array((32, 24, HEAD), BF16),
            array((8, 4, HEAD, HEAD), BF16),
            array((8, 8, WIDE), F32),
            array((32, WIDE), BF16),
        ]
        scratch += [pltpu.VMEM((8, 4, HEAD, HEAD), F32), pltpu.VMEM((32, WIDE), BF16)]
    else:
        buf_specs = [any_spec()] * len(bufs)
        out_specs += [block(2, 4, HEAD, HEAD), block(2, 8, WIDE)]
        out_shape += [array((8, 4, HEAD, HEAD), F32), array((8, 8, WIDE), F32)]
    copies = 4 if last else 2
    aliased = min(len(bufs), 2 if last else 4)
    return pl.pallas_call(
        functools.partial(keys_kernel, first, last),
        grid_spec=pltpu.PrefetchScalarGridSpec(
            num_scalar_prefetch=2,
            grid=(1,),
            in_specs=[any_spec()] * 2
            + [whole(1, WIDE)]
            + [pl.BlockSpec((4, BLK), lambda i, t, p, k=k: (0, block_of(t, p, 2 * group + k))) for k in range(2)]
            + weight_specs
            + buf_specs,
            out_specs=out_specs,
            scratch_shapes=scratch + [pltpu.SemaphoreType.DMA((copies,))],
        ),
        out_shape=out_shape,
        input_output_aliases={11 + k: k for k in range(aliased)},
        compiler_params=params("last" if last else "keys"),
        cost_estimate=pl.CostEstimate(
            flops=2 * rows * depth * WIDE * 6, bytes_accessed=12 * 2**20, transcendentals=0
        ),
    )(t, jnp.asarray(PLACES), *x, gap, shift, shift, *weights, *bufs)


def prefix_kernel(packs, arriving):
    state = jnp.zeros((16, HEAD), F32)
    for i in range(32):
        arriving[i] = state.astype(BF16)
        tile = packs[i, 16:24, :].astype(F32)
        log = tile[0:1] + tile[1:2] + tile[2:3]
        state = jnp.exp(log) * state + packs[i, 0:16, :].astype(F32)


def arriving_states(pack):
    packs = lax.all_to_all(pack, "sp", split_axis=0, concat_axis=0, tiled=True)
    arriving = pl.pallas_call(
        prefix_kernel,
        out_shape=jax.ShapeDtypeStruct((32, 16, HEAD), BF16),
        compiler_params=params("prefix"),
        cost_estimate=pl.CostEstimate(flops=10**8, bytes_accessed=2**20, transcendentals=0),
        name="prefix",
    )(packs)
    arrived = lax.all_to_all(arriving, "sp", split_axis=0, concat_axis=0, tiled=True)
    return arrived.reshape(4, HEAD, HEAD)


def filter_kernel(t, places, mixed, halo, taps, filtered, stats, window, sums):
    i = pl.program_id(0)
    reach = 32

    @pl.when(i == 0)
    def _():
        window[0:reach, :] = halo[...].astype(F32)

    @pl.when(i > 0)
    def _():
        window[0:reach, :] = window[BLK : BLK + reach, :]

    window[reach : reach + BLK, :] = mixed[...].astype(F32)
    sums[...] = jnp.zeros_like(sums)

    def one(c, carry):
        lanes = pl.ds(pl.multiple_of(c * HEAD, HEAD), HEAD)
        acc = jnp.zeros((BLK, HEAD), F32)
        for r in range(8):
            used = [q for q in range(5) if 0 <= 8 * q + r - 2 < 31]
            shifted = window[8 * used[0] + r : 8 * used[-1] + r + BLK, lanes]
            part = None
            for q in used:
                j, lead = 8 * q + r - 2, 8 * (q - used[0])
                term = taps[j : j + 1, lanes] * shifted[lead : lead + BLK, :]
                part = term if part is None else part + term
            acc = acc + part
        filtered[:, lanes] = acc
        sums[0] = sums[0] + acc
        sums[1] = sums[1] + acc * acc
        return carry

    lax.fori_loop(0, 4, one, 0)
    lane = lax.broadcasted_iota(jnp.int32, (BLK, HEAD), 1)
    tile = jnp.where(
        lane == 0,
        jnp.sum(sums[0], axis=1, keepdims=True),
        jnp.where(lane == 1, jnp.sum(sums[1], axis=1, keepdims=True), 0.0),
    )
    stats[...] = jnp.transpose(tile)[0:8, :]


def filter_rows(t, mixed, halo, taps):
    return pl.pallas_call(
        filter_kernel,
        grid_spec=pltpu.PrefetchScalarGridSpec(
            num_scalar_prefetch=2,
            grid=(8,),
            in_specs=[
                pl.BlockSpec((BLK, WIDE), lambda i, t, p: (slot_of(t, p, i), 0)),
                pl.BlockSpec((32, WIDE), lambda i, t, p: (0, 0)),
                pl.BlockSpec((31, WIDE), lambda i, t, p: (0, 0)),
            ],
            out_specs=[
                pl.BlockSpec((BLK, WIDE), lambda i, t, p: (slot_of(t, p, i), 0)),
                pl.BlockSpec((8, BLK), lambda i, t, p: (0, i)),
            ],
            scratch_shapes=[pltpu.VMEM((32 + BLK, WIDE), F32), pltpu.VMEM((2, BLK, HEAD), F32)],
        ),
        out_shape=[
            jax.ShapeDtypeStruct((8 * BLK, WIDE), F32),
            jax.ShapeDtypeStruct((8, 8 * BLK), F32),
        ],
        compiler_params=params("filter"),
        cost_estimate=pl.CostEstimate(flops=7 * 10**9, bytes_accessed=5 * 2**20, transcendentals=0),
        name="filter_rows",
    )(t, jnp.asarray(PLACES), mixed, halo, taps)


QUERY_SCRATCH = [((2 * BLK, 2048), BF16), ((2, 2048, WIDE), BF16), ((2 * BLK, 2 * WIDE), BF16), ((2 * BLK, WIDE), BF16)]
NEAR_SCRATCH = [((2 * BLK, WIDE), F32), ((2 * BLK, WIDE), BF16), ((2 * BLK, WIDE), BF16)]


def rows_of(ref, group, size):
    return ref.at[pl.ds(group * size, size)]


def query_side(group, later, ins, scratch, outs, sems):
    x_top, x_bottom, fv_all, w_query, w_rgate, gap, *shifts = ins
    xbuf, wbuf, fv, query = scratch
    near, query_near, rgate = outs
    copies = fetch(
        [
            (x_top, xbuf.at[pl.ds(0, BLK)]),
            (x_bottom, xbuf.at[pl.ds(BLK, BLK)]),
            (w_query, wbuf.at[0]),
            (rows_of(fv_all, group, 2 * BLK), fv),
            (w_rgate, wbuf.at[1]),
        ],
        sems,
    )
    for k in range(3):
        copies[k].wait()
    more = later()
    query[...] = dot(xbuf[...], wbuf[0]).astype(BF16)
    copies[3].wait()
    for k, shift in enumerate(shifts):
        rows = slice(k * BLK, (k + 1) * BLK)
        key, run = gates(fv[rows, 0:WIDE], gap[...], shift[...])
        block_outputs(key, run, fv[rows, WIDE : 2 * WIDE], query[rows, :], near, query_near, rows)
    copies[4].wait()
    rgate[...] = dot(xbuf[...], wbuf[1]).astype(BF16)
    return more


def query_kernel(group, t, places, *refs):
    outs, scratch, sems = refs[8:11], refs[11:15], refs[15]
    query_side(group, lambda: None, refs[:8], scratch, outs, sems)


def query_specs(group):
    return (
        [hbm_spec()] * 5
        + [pl.BlockSpec((1, WIDE), lambda i, t, p: (0, 0))]
        + [pl.BlockSpec((4, BLK), lambda i, t, p, k=k: (0, block_of(t, p, 2 * group + k))) for k in range(2)]
    )


def query_rows(group, x, t, fv, gap, shift, w_query, w_rgate):
    return pl.pallas_call(
        functools.partial(query_kernel, group),
        grid_spec=pltpu.PrefetchScalarGridSpec(
            num_scalar_prefetch=2,
            grid=(1,),
            in_specs=query_specs(group),
            out_specs=[pl.BlockSpec((2 * BLK, WIDE), lambda i, t, p: (0, 0))] * 3,
            scratch_shapes=[pltpu.VMEM(*v) for v in QUERY_SCRATCH] + [pltpu.SemaphoreType.DMA((5,))],
        ),
        out_shape=[jax.ShapeDtypeStruct((2 * BLK, WIDE), kind) for kind in (F32, BF16, BF16)],
        compiler_params=params("query"),
        cost_estimate=pl.CostEstimate(
            flops=2 * 2 * BLK * 2048 * WIDE * 4, bytes_accessed=6 * 2**20, transcendentals=0
        ),
    )(t, jnp.asarray(PLACES), *x, fv, w_query, w_rgate, gap, shift, shift)


MERGE_SCRATCH = [
    ((2, WIDE, 2048), BF16),
    ((2, 4, HEAD, HEAD), BF16),
    ((2, 8, WIDE), F32),
    ((4, HEAD, HEAD), BF16),
    ((2 * BLK, WIDE), F32),
    ((4, 8, 8 * BLK), F32),
    ((2 * BLK, 2 * WIDE), BF16),
]


def merge_kernel(group, split, t, places, *refs):
    lead, refs = (refs[:3], refs[3:]) if split else (refs[:8], refs[8:])
    starts_all, offsets_all, arrived_all, filtered_all, *stats_all = refs[:8]
    w_rec, w_conv, head_gain, conv_gain, top, bottom = refs[8:14]
    obuf, starts, offsets, arrived, filtered, stats_buf, act = refs[14:21]
    near, query_near, rgate = refs[21:24]
    sems, refs = refs[24], refs[25:]

    def later():
        return fetch(
            [
                (rows_of(starts_all, group, 2), starts),
                (rows_of(offsets_all, group, 2), offsets),
                (arrived_all, arrived),
                (rows_of(filtered_all, group, 2 * BLK), filtered),
            ]
            + [(s, stats_buf.at[k]) for k, s in enumerate(stats_all)]
            + [(w_rec, obuf.at[0]), (w_conv, obuf.at[1])],
            sems,
        )

    if split:
        first = fetch(list(zip(lead, (near, query_near, rgate))), refs[0])
        more = later()
        for copy in first:
            copy.wait()
    else:
        more = query_side(group, later, lead, refs[:4], (near, query_near, rgate), refs[4])
    for copy in more[:8]:
        copy.wait()
    for k in range(2):
        rows = slice(k * BLK, (k + 1) * BLK)
        carry = jnp.exp(offsets[k, 0:1, :])
        for h in range(4):
            lanes = slice(h * HEAD, (h + 1) * HEAD)
            state = starts[k, h].astype(F32) + carry[:, lanes] * arrived[h].astype(F32)
            rec = near[rows, lanes] + dot(query_near[rows, lanes], state.astype(BF16), ((1,), (1,)))
            rec = rec * lax.rsqrt(jnp.mean(rec * rec, axis=-1, keepdims=True) + HEAD_EPS)
            rec = rec * head_gain[...] * silu(rgate[rows, lanes].astype(F32))
            act[rows, lanes] = rec.astype(BF16)
        at = pl.ds(pl.multiple_of(block_of(t, places, 2 * group + k) * BLK, BLK), BLK)
        stats = (stats_buf[0, :, at] + stats_buf[1, :, at]) + (stats_buf[2, :, at] + stats_buf[3, :, at])
        tile = jnp.transpose(jnp.concatenate([stats] * 16, axis=0))
        mean = tile[:, 0:1] / 2048.0
        scale = lax.rsqrt(tile[:, 1:2] / 2048.0 - mean * mean + NORM_EPS)
        normed = (filtered[rows, :] - mean) * scale * conv_gain[...]
        act[rows, WIDE : 2 * WIDE] = silu(normed).astype(BF16)
    more[8].wait()
    more[9].wait()
    for n in range(4):
        cols = slice(n * 512, (n + 1) * 512)
        part = dot(act[:, 0:WIDE], obuf[0, :, cols]) + dot(act[:, WIDE : 2 * WIDE], obuf[1, :, cols])
        top[:, cols] = part[0:BLK, :].astype(BF16)
        bottom[:, cols] = part[BLK : 2 * BLK, :].astype(BF16)


def merge(group, x, t, fv, gap, shift, starts, offsets, arrived, head_gain, filtered, stats, conv_gain, w_query, w_rgate, out_rec, out_conv, ready=None):
    width = out_rec.shape[1]
    split = ready is not None
    whole = lambda *shape: pl.BlockSpec(shape, lambda i, t, p: (0,) * len(shape))
    scratch = [pltpu.VMEM(*v) for v in MERGE_SCRATCH + NEAR_SCRATCH] + [pltpu.SemaphoreType.DMA((10,))]
    if split:
        lead, lead_specs = ready, [hbm_spec()] * 3
        scratch += [pltpu.SemaphoreType.DMA((3,))]
    else:
        lead, lead_specs = (*x, fv, w_query, w_rgate, gap, shift, shift), query_specs(group)
        scratch += [pltpu.VMEM(*v) for v in QUERY_SCRATCH] + [pltpu.SemaphoreType.DMA((5,))]
    return pl.pallas_call(
        functools.partial(merge_kernel, group, split),
        grid_spec=pltpu.PrefetchScalarGridSpec(
            num_scalar_prefetch=2,
            grid=(1,),
            in_specs=lead_specs + [hbm_spec()] * 10 + [whole(1, HEAD), whole(1, WIDE)],
            out_specs=[whole(BLK, width), whole(BLK, width)],
            scratch_shapes=scratch,
        ),
        out_shape=[jax.ShapeDtypeStruct((BLK, width), BF16)] * 2,
        compiler_params=params({3: "merge_3", 0: "merge_0"}.get(group, "merge")),
        cost_estimate=pl.CostEstimate(
            flops=2 * 2 * BLK * 1024 * 2048 * 6, bytes_accessed=10 * 2**20, transcendentals=0
        ),
    )(t, jnp.asarray(PLACES), *lead, starts, offsets, arrived, filtered, *stats, out_rec, out_conv, head_gain, conv_gain)


def permuted(value, perm):
    return lax.ppermute(value, "tp", perm)


def on_device(
    tokens,
    norm_gain,
    w_query,
    w_forget,
    w_value,
    w_rgate,
    w_glu_value,
    w_glu_gate,
    forget_gap,
    decay_shift,
    head_gain,
    conv_taps,
    conv_gain,
    out_rec,
    out_conv,
):
    ahead = [(i, (i + 1) % 4) for i in range(4)]
    behind = [(i, (i - 1) % 4) for i in range(4)]
    t = lax.axis_index("tp").astype(jnp.int32).reshape(1)
    gap, shift = forget_gap[None, :], decay_shift.T
    a, b = norm_rows(tokens, norm_gain[None, :])
    from_back_a = permuted(a, ahead)
    from_front_b = permuted(b, behind)
    from_back_b = permuted(b, ahead)
    from_front_a = permuted(a, behind)
    far_a = permuted(from_back_a, ahead)
    far_b = permuted(from_front_b, behind)
    slots = ((a, b), (from_back_a, from_front_b), (from_back_b, from_front_a), (far_a, far_b))

    weights = (w_forget, w_value, w_glu_value, w_glu_gate)
    bufs = ()
    for group in range(3):
        bufs = keys(group, slots[group], t, gap, shift, weights, bufs)
    fv, mixed, pack, starts, offsets, edge = keys(3, slots[3], t, gap, shift, weights, bufs)

    halo = lax.ppermute(edge, "sp", [(i, i + 1) for i in range(31)])
    arrived = arriving_states(pack)
    filtered, stats = filter_rows(t, mixed, halo, conv_taps)
    stats_all = [stats] + [permuted(stats, [(i, (i + d) % 4) for i in range(4)]) for d in (1, 2, 3)]
    ready = query_rows(3, slots[3], t, fv, gap, shift, w_query, w_rgate)

    part = functools.partial(
        merge, t=t, fv=fv, gap=gap, shift=shift, starts=starts, offsets=offsets, arrived=arrived,
        head_gain=head_gain[None, :], filtered=filtered, stats=stats_all, conv_gain=conv_gain[None, :],
        w_query=w_query, w_rgate=w_rgate, out_rec=out_rec, out_conv=out_conv,
    )
    add = lambda x, y: (x.astype(F32) + y.astype(F32)).astype(BF16)
    far_top, far_bottom = part(3, slots[3], ready=ready)
    via_back = permuted(far_top, ahead)
    via_front = permuted(far_bottom, behind)
    back_a, front_b = part(1, slots[1])
    got_b = permuted(front_b, ahead)
    got_a = permuted(back_a, behind)
    back_b, front_a = part(2, slots[2])
    sum_a = permuted(add(front_a, via_back), ahead)
    sum_b = permuted(add(back_b, via_front), behind)
    own_a, own_b = part(0, slots[0])
    wide = lambda x: x.astype(F32)
    ready = jnp.concatenate([wide(own_a) + wide(got_a), wide(own_b) + wide(got_b)], axis=0)
    ready = lax.optimization_barrier(ready)
    return (ready + wide(jnp.concatenate([sum_a, sum_b], axis=0))).astype(BF16)


def solution(mesh):
    placed = (
        P(("sp", "tp"), None),
        P(),
        P(None, "tp"),
        P(None, "tp"),
        P(None, "tp"),
        P(None, "tp"),
        P(None, "tp"),
        P(None, "tp"),
        P("tp"),
        P("sp", "tp"),
        P(),
        P(None, "tp"),
        P("tp"),
        P("tp", None),
        P("tp", None),
    )
    return jax.shard_map(on_device, mesh=mesh, in_specs=placed, out_specs=P(("sp", "tp"), None), check_vma=False)
```

```python
import functools

import jax
import jax.numpy as jnp
import numpy as np
from jax import lax
from jax.experimental import pallas as pl
from jax.experimental.pallas import tpu as pltpu
from jax.sharding import PartitionSpec as P


HEAD = 128
BLK = 128
NORM_EPS = 1e-05
HEAD_EPS = 1e-06
F32 = jnp.float32
BF16 = jnp.bfloat16


SLOT = np.array([[0, 1], [5, 3], [6, 7], [2, 4]])
SLOT_TABLE = np.array(
    [[SLOT[(p // 2 - t) % 4][p % 2] for p in range(8)] for t in range(4)], dtype=np.int32
)
PLACE_TABLE = np.argsort(SLOT_TABLE, axis=1).astype(np.int32)
PLACES = np.concatenate([PLACE_TABLE, SLOT_TABLE], axis=1).reshape(-1)


def block_of(t, places, slot):
    return places[16 * t[0] + slot]


def slot_of(t, places, block):
    return places[16 * t[0] + 8 + block]


LIMITS = {"norm": 58, "keys": 28, "last": 28, "filter": 58, "prefix": 50, "query": 58, "merge_3": 16, "merge": 24, "merge_0": 24}


def params(kind):
    return pltpu.CompilerParams(vmem_limit_bytes=LIMITS[kind] * 1024 * 1024)


def dot(a, b, dims=((1,), (0,))):
    return lax.dot_general(a, b, (dims, ((), ())), preferred_element_type=F32)


def silu(x):
    return x * jax.nn.sigmoid(x)


WIDE = 4 * HEAD


def gates(forget, gap, shift):
    key = gap * jax.nn.sigmoid(-forget.astype(F32))
    columns = jnp.transpose(jnp.concatenate([shift] * (BLK // 4), axis=0))
    spread = jnp.concatenate(
        [jnp.broadcast_to(columns[:, h : h + 1], (BLK, HEAD)) for h in range(4)], axis=1
    )
    log_forget = jnp.log1p(-key) + spread
    high = log_forget.astype(BF16)
    low = (log_forget - high.astype(F32)).astype(BF16)
    rows = lax.broadcasted_iota(jnp.int32, (BLK, BLK), 0)
    cols = lax.broadcasted_iota(jnp.int32, (BLK, BLK), 1)
    lower = (rows >= cols).astype(F32).astype(BF16)
    return key, dot(lower, high) + dot(lower, low)


def pieces(log_row):
    high = log_row.astype(BF16).astype(F32)
    mid = (log_row - high).astype(BF16).astype(F32)
    low = log_row - high - mid
    row = lax.broadcasted_iota(jnp.int32, (16, HEAD), 0)
    tile = jnp.where(row == 0, high, jnp.where(row == 1, mid, jnp.where(row == 2, low, 0.0)))
    return tile.astype(BF16)


def block_outputs(key, run, value, query, near, query_near, at):
    middle = run[BLK // 2 - 1 : BLK // 2, :]
    query_mid = silu(query.astype(F32)) * jnp.exp(run - middle)
    key_mid = (key * jnp.exp(middle - run)).astype(BF16)
    query_near[at, :] = (query_mid * jnp.exp(middle)).astype(BF16)
    query_mid = query_mid.astype(BF16)
    rows = lax.broadcasted_iota(jnp.int32, (BLK, BLK), 0)
    cols = lax.broadcasted_iota(jnp.int32, (BLK, BLK), 1)
    for h in range(4):
        lanes = slice(h * HEAD, (h + 1) * HEAD)
        scores = dot(query_mid[:, lanes], key_mid[:, lanes], ((1,), (1,)))
        scores = jnp.where(rows >= cols, scores, 0.0).astype(BF16)
        near[at, lanes] = dot(scores, value[:, lanes])


def fetch(pairs, sems):
    copies = [pltpu.make_async_copy(source, target, sems.at[k]) for k, (source, target) in enumerate(pairs)]
    for copy in copies:
        copy.start()
    return copies


def norm_kernel(tokens, gain, top, bottom, rows_in, gain_in, rows_out, sems, out_sems):
    halves = [pl.ds(0, BLK), pl.ds(BLK, BLK)]
    copies = fetch([(gain, gain_in)] + [(tokens.at[h], rows_in.at[h]) for h in halves], sems)
    copies[0].wait()
    g = gain_in[...]
    sends = []
    for k, out in enumerate((top, bottom)):
        copies[1 + k].wait()
        for r in range(k * BLK, (k + 1) * BLK, 16):
            rows = rows_in[r : r + 16, :].astype(F32)
            centred = rows - jnp.mean(rows, axis=-1, keepdims=True)
            var = jnp.mean(centred * centred, axis=-1, keepdims=True)
            rows_out[r : r + 16, :] = (centred * lax.rsqrt(var + NORM_EPS) * g).astype(BF16)
        send = pltpu.make_async_copy(rows_out.at[halves[k]], out, out_sems.at[k])
        send.start()
        sends.append(send)
    for send in sends:
        send.wait()


def norm_rows(tokens, gain):
    half = jax.ShapeDtypeStruct((BLK, tokens.shape[1]), BF16)
    return pl.pallas_call(
        norm_kernel,
        in_specs=[hbm_spec()] * 2,
        out_specs=[any_spec()] * 2,
        out_shape=[half, half],
        scratch_shapes=[
            pltpu.VMEM(tokens.shape, BF16),
            pltpu.VMEM(gain.shape, F32),
            pltpu.VMEM(tokens.shape, BF16),
            pltpu.SemaphoreType.DMA((3,)),
            pltpu.SemaphoreType.DMA((2,)),
        ],
        compiler_params=params("norm"),
        name="norm_rows",
    )(tokens, gain)


def glu(value, gate):
    return (value.astype(F32) * jax.nn.sigmoid(gate.astype(F32))).astype(BF16)


def keys_kernel(first, last, t, places, *refs):
    x_top, x_bottom, gap, shift_top, shift_bottom = refs[:5]
    weights, refs = refs[5:9], refs[9:]
    if first:
        fv, mixed, added, close, xbuf, sems = refs
    elif last:
        mixed_in, added, close_all, fv, mixed, pack, starts, offsets, edge, xbuf, parts, tail, sems = refs[1:]
    else:
        fv, mixed, added, close, xbuf, sems = refs[4:]
    pairs = [(x_top, xbuf.at[pl.ds(0, BLK)]), (x_bottom, xbuf.at[pl.ds(BLK, BLK)])]
    if last:
        tail_slot = slot_of(t, places, 7)
        start = pl.multiple_of(jnp.minimum(tail_slot, 5) * BLK + BLK - 32, 32)
        pairs += [(added.at[pl.ds(0, 6)], parts.at[pl.ds(0, 6)]), (mixed_in.at[pl.ds(start, 32)], tail)]
    copies = fetch(pairs, sems)
    copies[0].wait()
    copies[1].wait()

    def times(n):
        return dot(xbuf[...], weights[n][...]).astype(BF16)

    fv[:, 0:WIDE] = times(0)
    fv[:, WIDE : 2 * WIDE] = times(1)
    ends = []
    for k, shift in enumerate((shift_top, shift_bottom)):
        at = slice(k * BLK, (k + 1) * BLK)
        key, run = gates(fv[at, 0:WIDE], gap[...], shift[...])
        value = fv[at, WIDE : 2 * WIDE]
        end = run[BLK - 1 : BLK, :]
        key_far = (key * jnp.exp(end - run)).astype(BF16)
        ends.append(end)
        if not last:
            close[k] = jnp.broadcast_to(end, (8, WIDE))
        for h in range(4):
            lanes = slice(h * HEAD, (h + 1) * HEAD)
            sum_h = dot(value[:, lanes], key_far[:, lanes], ((0,), (0,)))
            if last:
                parts[6 + k, h] = sum_h
            else:
                added[k, h] = sum_h
    mixed_now = glu(times(2), times(3))
    mixed[...] = mixed_now
    if last:
        copies[2].wait()
        copies[3].wait()
        edge[...] = jnp.where(
            tail_slot == 7, mixed_now[2 * BLK - 32 :, :].astype(F32), tail[...].astype(F32)
        ).astype(BF16)
        scan_blocks(t, places, ends, close_all, parts, pack, starts, offsets)


def scan_blocks(t, places, ends, close_all, parts, pack, starts, offsets):
    state = [jnp.zeros((HEAD, HEAD), F32) for _ in range(4)]
    total = jnp.zeros((1, WIDE), F32)
    for i in range(8):
        slot = slot_of(t, places, i)
        offsets[slot] = jnp.broadcast_to(total, (8, WIDE))
        end = jnp.where(
            slot == 6, ends[0], jnp.where(slot == 7, ends[1], close_all[jnp.minimum(slot, 5)][0:1, :])
        )
        keep = jnp.exp(end)
        for h in range(4):
            lanes = slice(h * HEAD, (h + 1) * HEAD)
            starts[slot, h] = state[h].astype(BF16)
            state[h] = state[h] * keep[:, lanes] + parts[slot, h]
        total = total + end
    for h in range(4):
        tile = pieces(total[:, h * HEAD : (h + 1) * HEAD])
        rows = state[h].astype(BF16)
        for j in range(8):
            pack[8 * h + j, 0:16, :] = rows[16 * j : 16 * j + 16, :]
            pack[8 * h + j, 16:24, :] = tile[0:8, :]


def any_spec():
    return pl.BlockSpec(memory_space=pl.ANY)


def hbm_spec():
    return pl.BlockSpec(memory_space=pltpu.HBM)


def keys(group, x, t, gap, shift, weights, bufs):
    depth = x[0].shape[1]
    rows = 2 * BLK
    first, last = group == 0, group == 3
    block = lambda *shape: pl.BlockSpec(shape, lambda i, t, p: (group,) + (0,) * (len(shape) - 1))
    whole = lambda *shape: pl.BlockSpec(shape, lambda i, t, p: (0,) * len(shape))
    array = jax.ShapeDtypeStruct
    out_specs = [block(rows, 2 * WIDE), block(rows, WIDE)]
    out_shape = [array((8 * BLK, 2 * WIDE), BF16), array((8 * BLK, WIDE), BF16)]
    scratch = [pltpu.VMEM((rows, depth), BF16)]
    weight_specs = [pl.BlockSpec(memory_space=pltpu.VMEM)] * 4
    if last:
        buf_specs = [any_spec(), any_spec(), any_spec(), whole(8, 8, WIDE)]
        out_specs += [whole(32, 24, HEAD), whole(8, 4, HEAD, HEAD), whole(8, 8, WIDE), whole(32, WIDE)]
        out_shape += [
            array((32, 24, HEAD), BF16),
            array((8, 4, HEAD, HEAD), BF16),
            array((8, 8, WIDE), F32),
            array((32, WIDE), BF16),
        ]
        scratch += [pltpu.VMEM((8, 4, HEAD, HEAD), F32), pltpu.VMEM((32, WIDE), BF16)]
    else:
        buf_specs = [any_spec()] * len(bufs)
        out_specs += [block(2, 4, HEAD, HEAD), block(2, 8, WIDE)]
        out_shape += [array((8, 4, HEAD, HEAD), F32), array((8, 8, WIDE), F32)]
    copies = 4 if last else 2
    aliased = min(len(bufs), 2 if last else 4)
    return pl.pallas_call(
        functools.partial(keys_kernel, first, last),
        grid_spec=pltpu.PrefetchScalarGridSpec(
            num_scalar_prefetch=2,
            grid=(1,),
            in_specs=[any_spec()] * 2
            + [whole(1, WIDE)]
            + [pl.BlockSpec((4, BLK), lambda i, t, p, k=k: (0, block_of(t, p, 2 * group + k))) for k in range(2)]
            + weight_specs
            + buf_specs,
            out_specs=out_specs,
            scratch_shapes=scratch + [pltpu.SemaphoreType.DMA((copies,))],
        ),
        out_shape=out_shape,
        input_output_aliases={11 + k: k for k in range(aliased)},
        compiler_params=params("last" if last else "keys"),
        cost_estimate=pl.CostEstimate(
            flops=2 * rows * depth * WIDE * 6, bytes_accessed=12 * 2**20, transcendentals=0
        ),
    )(t, jnp.asarray(PLACES), *x, gap, shift, shift, *weights, *bufs)


def prefix_kernel(packs, arriving):
    state = jnp.zeros((16, HEAD), F32)
    for i in range(32):
        arriving[i] = state.astype(BF16)
        tile = packs[i, 16:24, :].astype(F32)
        log = tile[0:1] + tile[1:2] + tile[2:3]
        state = jnp.exp(log) * state + packs[i, 0:16, :].astype(F32)


def arriving_states(pack):
    packs = lax.all_to_all(pack, "sp", split_axis=0, concat_axis=0, tiled=True)
    arriving = pl.pallas_call(
        prefix_kernel,
        out_shape=jax.ShapeDtypeStruct((32, 16, HEAD), BF16),
        compiler_params=params("prefix"),
        cost_estimate=pl.CostEstimate(flops=10**8, bytes_accessed=2**20, transcendentals=0),
        name="prefix",
    )(packs)
    arrived = lax.all_to_all(arriving, "sp", split_axis=0, concat_axis=0, tiled=True)
    return arrived.reshape(4, HEAD, HEAD)


def filter_kernel(t, places, mixed_a, mixed_b, halo, taps, filtered, stats, window, sums):
    i = pl.program_id(0)
    reach = 32

    @pl.when(i == 0)
    def _():
        window[0:reach, :] = halo[...].astype(F32)

    @pl.when(i > 0)
    def _():
        window[0:reach, :] = window[2 * BLK : 2 * BLK + reach, :]

    window[reach : reach + BLK, :] = mixed_a[...].astype(F32)
    window[reach + BLK : reach + 2 * BLK, :] = mixed_b[...].astype(F32)
    sums[...] = jnp.zeros_like(sums)

    def one(n, carry):
        lanes = pl.ds(pl.multiple_of(lax.rem(n, 4) * HEAD, HEAD), HEAD)
        half = lax.div(n, 4)
        base = half * BLK
        acc = jnp.zeros((BLK, HEAD), F32)
        for r in range(8):
            used = [q for q in range(5) if 0 <= 8 * q + r - 2 < 31]
            reads = window[pl.ds(pl.multiple_of(base, BLK), BLK + 40), lanes]
            shifted = reads[8 * used[0] + r : 8 * used[-1] + r + BLK, :]
            part = None
            for q in used:
                j, lead = 8 * q + r - 2, 8 * (q - used[0])
                term = taps[j : j + 1, lanes] * shifted[lead : lead + BLK, :]
                part = term if part is None else part + term
            acc = acc + part
        filtered[pl.ds(pl.multiple_of(base, BLK), BLK), lanes] = acc
        sums[half, 0] = sums[half, 0] + acc
        sums[half, 1] = sums[half, 1] + acc * acc
        return carry

    lax.fori_loop(0, 8, one, 0)
    lane = lax.broadcasted_iota(jnp.int32, (BLK, HEAD), 1)
    for half in range(2):
        tile = jnp.where(
            lane == 0,
            jnp.sum(sums[half, 0], axis=1, keepdims=True),
            jnp.where(lane == 1, jnp.sum(sums[half, 1], axis=1, keepdims=True), 0.0),
        )
        stats[:, half * BLK : (half + 1) * BLK] = jnp.transpose(tile)[0:8, :]


def filter_rows(t, mixed, halo, taps):
    return pl.pallas_call(
        filter_kernel,
        grid_spec=pltpu.PrefetchScalarGridSpec(
            num_scalar_prefetch=2,
            grid=(4,),
            in_specs=[
                pl.BlockSpec((BLK, WIDE), lambda i, t, p: (slot_of(t, p, 2 * i), 0)),
                pl.BlockSpec((BLK, WIDE), lambda i, t, p: (slot_of(t, p, 2 * i + 1), 0)),
                pl.BlockSpec((32, WIDE), lambda i, t, p: (0, 0)),
                pl.BlockSpec((31, WIDE), lambda i, t, p: (0, 0)),
            ],
            out_specs=[
                pl.BlockSpec((2 * BLK, WIDE), lambda i, t, p: (i, 0)),
                pl.BlockSpec((8, 2 * BLK), lambda i, t, p: (0, i)),
            ],
            scratch_shapes=[
                pltpu.VMEM((40 + 2 * BLK, WIDE), F32),
                pltpu.VMEM((2, 2, BLK, HEAD), F32),
            ],
        ),
        out_shape=[
            jax.ShapeDtypeStruct((8 * BLK, WIDE), F32),
            jax.ShapeDtypeStruct((8, 8 * BLK), F32),
        ],
        compiler_params=params("filter"),
        cost_estimate=pl.CostEstimate(flops=7 * 10**9, bytes_accessed=5 * 2**20, transcendentals=0),
        name="filter_rows",
    )(t, jnp.asarray(PLACES), mixed, mixed, halo, taps)


QUERY_SCRATCH = [((2 * BLK, 2048), BF16), ((2, 2048, WIDE), BF16), ((2 * BLK, 2 * WIDE), BF16), ((2 * BLK, WIDE), BF16)]
NEAR_SCRATCH = [((2 * BLK, WIDE), F32), ((2 * BLK, WIDE), BF16), ((2 * BLK, WIDE), BF16)]


def rows_of(ref, group, size):
    return ref.at[pl.ds(group * size, size)]


def query_side(group, later, ins, scratch, outs, sems):
    x_top, x_bottom, fv_all, w_query, w_rgate, gap, *shifts = ins
    xbuf, wbuf, fv, query = scratch
    near, query_near, rgate = outs
    copies = fetch(
        [
            (x_top, xbuf.at[pl.ds(0, BLK)]),
            (x_bottom, xbuf.at[pl.ds(BLK, BLK)]),
            (w_query, wbuf.at[0]),
            (rows_of(fv_all, group, 2 * BLK), fv),
            (w_rgate, wbuf.at[1]),
        ],
        sems,
    )
    for k in range(3):
        copies[k].wait()
    more = later()
    query[...] = dot(xbuf[...], wbuf[0]).astype(BF16)
    copies[3].wait()
    for k, shift in enumerate(shifts):
        rows = slice(k * BLK, (k + 1) * BLK)
        key, run = gates(fv[rows, 0:WIDE], gap[...], shift[...])
        block_outputs(key, run, fv[rows, WIDE : 2 * WIDE], query[rows, :], near, query_near, rows)
    copies[4].wait()
    rgate[...] = dot(xbuf[...], wbuf[1]).astype(BF16)
    return more


def query_kernel(group, t, places, *refs):
    out, scratch, sems, rest = refs[8], refs[9:13], refs[13], refs[14:]
    near = out.at[:, pl.ds(0, WIDE)]
    query_side(group, lambda: None, refs[:8], scratch, (near, *rest), sems)
    for k, ref in enumerate(rest):
        out[:, (k + 1) * WIDE : (k + 2) * WIDE] = ref[...].astype(F32)


def query_specs(group):
    return (
        [hbm_spec()] * 5
        + [pl.BlockSpec((1, WIDE), lambda i, t, p: (0, 0))]
        + [pl.BlockSpec((4, BLK), lambda i, t, p, k=k: (0, block_of(t, p, 2 * group + k))) for k in range(2)]
    )


def query_rows(group, x, t, fv, gap, shift, w_query, w_rgate):
    return pl.pallas_call(
        functools.partial(query_kernel, group),
        grid_spec=pltpu.PrefetchScalarGridSpec(
            num_scalar_prefetch=2,
            grid=(1,),
            in_specs=query_specs(group),
            out_specs=pl.BlockSpec((2 * BLK, 3 * WIDE), lambda i, t, p: (0, 0)),
            scratch_shapes=[pltpu.VMEM(*v) for v in QUERY_SCRATCH]
            + [pltpu.SemaphoreType.DMA((5,))]
            + [pltpu.VMEM(*v) for v in NEAR_SCRATCH[1:]],
        ),
        out_shape=jax.ShapeDtypeStruct((2 * BLK, 3 * WIDE), F32),
        compiler_params=params("query"),
        cost_estimate=pl.CostEstimate(
            flops=2 * 2 * BLK * 2048 * WIDE * 4, bytes_accessed=6 * 2**20, transcendentals=0
        ),
    )(t, jnp.asarray(PLACES), *x, fv, w_query, w_rgate, gap, shift, shift)


MERGE_SCRATCH = [
    ((2, WIDE, 2048), BF16),
    ((2, 4, HEAD, HEAD), BF16),
    ((2, 8, WIDE), F32),
    ((4, HEAD, HEAD), BF16),
    ((2 * BLK, WIDE), F32),
    ((4, 8, 8 * BLK), F32),
    ((2 * BLK, 2 * WIDE), BF16),
]


def merge_kernel(group, split, t, places, *refs):
    lead, refs = (refs[:1], refs[1:]) if split else (refs[:8], refs[8:])
    starts_all, offsets_all, arrived_all, filtered_all, *stats_all = refs[:8]
    w_rec, w_conv, head_gain, conv_gain, top, bottom = refs[8:14]
    obuf, starts, offsets, arrived, filtered, stats_buf, act = refs[14:21]
    if split:
        ready, sems, refs = refs[21], refs[22], refs[23:]
        near, query_near, rgate = (ready.at[:, pl.ds(k * WIDE, WIDE)] for k in range(3))
    else:
        near, query_near, rgate = refs[21:24]
        sems, refs = refs[24], refs[25:]

    def later():
        return fetch(
            [
                (rows_of(starts_all, group, 2), starts),
                (rows_of(offsets_all, group, 2), offsets),
                (arrived_all, arrived),
            ]
            + [
                (
                    filtered_all.at[pl.ds(pl.multiple_of(block_of(t, places, 2 * group + k) * BLK, BLK), BLK)],
                    filtered.at[pl.ds(k * BLK, BLK)],
                )
                for k in range(2)
            ]
            + [(s, stats_buf.at[k]) for k, s in enumerate(stats_all)]
            + [(w_rec, obuf.at[0]), (w_conv, obuf.at[1])],
            sems,
        )

    if split:
        first = fetch([(lead[0], ready)], refs[0])
        more = later()
        for copy in first:
            copy.wait()
    else:
        more = query_side(group, later, lead, refs[:4], (near, query_near, rgate), refs[4])
    for copy in more[:9]:
        copy.wait()
    for k in range(2):
        rows = slice(k * BLK, (k + 1) * BLK)
        carry = jnp.exp(offsets[k, 0:1, :])
        for h in range(4):
            lanes = slice(h * HEAD, (h + 1) * HEAD)
            state = starts[k, h].astype(F32) + carry[:, lanes] * arrived[h].astype(F32)
            rec = near[rows, lanes] + dot(query_near[rows, lanes].astype(BF16), state.astype(BF16), ((1,), (1,)))
            rec = rec * lax.rsqrt(jnp.mean(rec * rec, axis=-1, keepdims=True) + HEAD_EPS)
            rec = rec * head_gain[...] * silu(rgate[rows, lanes].astype(F32))
            act[rows, lanes] = rec.astype(BF16)
        at = pl.ds(pl.multiple_of(block_of(t, places, 2 * group + k) * BLK, BLK), BLK)
        stats = (stats_buf[0, :, at] + stats_buf[1, :, at]) + (stats_buf[2, :, at] + stats_buf[3, :, at])
        tile = jnp.transpose(jnp.concatenate([stats] * 16, axis=0))
        mean = tile[:, 0:1] / 2048.0
        scale = lax.rsqrt(tile[:, 1:2] / 2048.0 - mean * mean + NORM_EPS)
        normed = (filtered[rows, :] - mean) * scale * conv_gain[...]
        act[rows, WIDE : 2 * WIDE] = silu(normed).astype(BF16)
    more[9].wait()
    more[10].wait()
    for n in range(4):
        cols = slice(n * 512, (n + 1) * 512)
        part = dot(act[:, 0:WIDE], obuf[0, :, cols]) + dot(act[:, WIDE : 2 * WIDE], obuf[1, :, cols])
        top[:, cols] = part[0:BLK, :].astype(BF16)
        bottom[:, cols] = part[BLK : 2 * BLK, :].astype(BF16)


def merge(group, x, t, fv, gap, shift, starts, offsets, arrived, head_gain, filtered, stats, conv_gain, w_query, w_rgate, out_rec, out_conv, ready=None):
    width = out_rec.shape[1]
    split = ready is not None
    whole = lambda *shape: pl.BlockSpec(shape, lambda i, t, p: (0,) * len(shape))
    tail = [((2 * BLK, 3 * WIDE), F32)] if split else NEAR_SCRATCH
    scratch = [pltpu.VMEM(*v) for v in MERGE_SCRATCH + tail] + [pltpu.SemaphoreType.DMA((11,))]
    if split:
        lead, lead_specs = (ready,), [hbm_spec()]
        scratch += [pltpu.SemaphoreType.DMA((1,))]
    else:
        lead, lead_specs = (*x, fv, w_query, w_rgate, gap, shift, shift), query_specs(group)
        scratch += [pltpu.VMEM(*v) for v in QUERY_SCRATCH] + [pltpu.SemaphoreType.DMA((5,))]
    return pl.pallas_call(
        functools.partial(merge_kernel, group, split),
        grid_spec=pltpu.PrefetchScalarGridSpec(
            num_scalar_prefetch=2,
            grid=(1,),
            in_specs=lead_specs + [hbm_spec()] * 10 + [whole(1, HEAD), whole(1, WIDE)],
            out_specs=[whole(BLK, width), whole(BLK, width)],
            scratch_shapes=scratch,
        ),
        out_shape=[jax.ShapeDtypeStruct((BLK, width), BF16)] * 2,
        compiler_params=params({3: "merge_3", 0: "merge_0"}.get(group, "merge")),
        cost_estimate=pl.CostEstimate(
            flops=2 * 2 * BLK * 1024 * 2048 * 6, bytes_accessed=10 * 2**20, transcendentals=0
        ),
    )(t, jnp.asarray(PLACES), *lead, starts, offsets, arrived, filtered, *stats, out_rec, out_conv, head_gain, conv_gain)


def permuted(value, perm):
    return lax.ppermute(value, "tp", perm)


def on_device(
    tokens,
    norm_gain,
    w_query,
    w_forget,
    w_value,
    w_rgate,
    w_glu_value,
    w_glu_gate,
    forget_gap,
    decay_shift,
    head_gain,
    conv_taps,
    conv_gain,
    out_rec,
    out_conv,
):
    ahead = [(i, (i + 1) % 4) for i in range(4)]
    behind = [(i, (i - 1) % 4) for i in range(4)]
    t = lax.axis_index("tp").astype(jnp.int32).reshape(1)
    gap, shift = forget_gap[None, :], decay_shift.T
    a, b = norm_rows(tokens, norm_gain[None, :])
    from_back_a = permuted(a, ahead)
    from_front_b = permuted(b, behind)
    from_back_b = permuted(b, ahead)
    from_front_a = permuted(a, behind)
    far_a = permuted(from_back_a, ahead)
    far_b = permuted(from_front_b, behind)
    slots = ((a, b), (from_back_a, from_front_b), (from_back_b, from_front_a), (far_a, far_b))

    weights = (w_forget, w_value, w_glu_value, w_glu_gate)
    bufs = ()
    for group in range(3):
        bufs = keys(group, slots[group], t, gap, shift, weights, bufs)
    fv, mixed, pack, starts, offsets, edge = keys(3, slots[3], t, gap, shift, weights, bufs)

    halo = lax.ppermute(edge, "sp", [(i, i + 1) for i in range(31)])
    arrived = arriving_states(pack)
    filtered, stats = filter_rows(t, mixed, halo, conv_taps)
    stats_all = [stats] + [permuted(stats, [(i, (i + d) % 4) for i in range(4)]) for d in (1, 2, 3)]
    ready = query_rows(3, slots[3], t, fv, gap, shift, w_query, w_rgate)

    part = functools.partial(
        merge, t=t, fv=fv, gap=gap, shift=shift, starts=starts, offsets=offsets, arrived=arrived,
        head_gain=head_gain[None, :], filtered=filtered, stats=stats_all, conv_gain=conv_gain[None, :],
        w_query=w_query, w_rgate=w_rgate, out_rec=out_rec, out_conv=out_conv,
    )
    add = lambda x, y: (x.astype(F32) + y.astype(F32)).astype(BF16)
    far_top, far_bottom = part(3, slots[3], ready=ready)
    via_back = permuted(far_top, ahead)
    via_front = permuted(far_bottom, behind)
    back_a, front_b = part(1, slots[1])
    got_b = permuted(front_b, ahead)
    got_a = permuted(back_a, behind)
    back_b, front_a = part(2, slots[2])
    sum_a = permuted(add(front_a, via_back), ahead)
    sum_b = permuted(add(back_b, via_front), behind)
    own_a, own_b = part(0, slots[0])
    wide = lambda x: x.astype(F32)
    ready = jnp.concatenate([wide(own_a) + wide(got_a), wide(own_b) + wide(got_b)], axis=0)
    ready = lax.optimization_barrier(ready.astype(BF16))
    return (wide(ready) + wide(jnp.concatenate([sum_a, sum_b], axis=0))).astype(BF16)


def solution(mesh):
    placed = (
        P(("sp", "tp"), None),
        P(),
        P(None, "tp"),
        P(None, "tp"),
        P(None, "tp"),
        P(None, "tp"),
        P(None, "tp"),
        P(None, "tp"),
        P("tp"),
        P("sp", "tp"),
        P(),
        P(None, "tp"),
        P("tp"),
        P("tp", None),
        P("tp", None),
    )
    return jax.shard_map(on_device, mesh=mesh, in_specs=placed, out_specs=P(("sp", "tp"), None), check_vma=False)
```
